512 devices in a mesh: dp: 4 (over x), kv: 64 (over z, y), tp: 2 (over core).
Axes of the slice: x: 4, y: 4, z: 16, core: 2. Of those that a mesh axis runs over, the one named last changes fastest.
Arguments:
- stream: bfloat16 [512, 2048], P('dp', ('kv', 'tp')), parts along dimension 0, may hold values from -40 to 40
- old_state: float32 [512, 8, 64, 128], P(('dp', 'kv'), 'tp'), parts along dimension 0, may hold values from -6 to 6
- decay_amounts: float32 [512, 512], P(('dp', 'kv'), 'tp'), parts along dimension 0, may hold values from 0.003 to 1
- first_gain: float32 [2048], replicated, may hold values from 0.1 to 1.9
- first_gate: bfloat16 [2048, 5632], P(None, ('kv', 'tp')), may hold values from -0.125 to 0.125
- first_up: bfloat16 [2048, 5632], P(None, ('kv', 'tp')), may hold values from -0.125 to 0.125
- first_down: bfloat16 [5632, 2048], P(('kv', 'tp')), may hold values from -0.078125 to 0.078125
- mixer_gain: float32 [2048], P('kv'), may hold values from 0.1 to 1.9
- query_weight: bfloat16 [2048, 512], P('kv', 'tp'), may hold values from -0.125 to 0.125
- key_weight: bfloat16 [2048, 512], P('kv', 'tp'), may hold values from -0.125 to 0.125
- decay_weight: bfloat16 [2048, 512], P('kv', 'tp'), may hold values from -0.5 to 0.5
- value_weight: bfloat16 [2048, 1024], P('kv', 'tp'), may hold values from -0.125 to 0.125
- output_gate_weight: bfloat16 [2048, 1024], P('kv', 'tp'), may hold values from -0.125 to 0.125
- head_gain: float32 [1024], P('tp'), may hold values from 0.1 to 1.9
- output_weight: bfloat16 [1024, 2048], P('tp', 'kv'), may hold values from -0.1875 to 0.1875
- second_gain: float32 [2048], replicated, may hold values from 0.1 to 1.9
- second_gate: bfloat16 [2048, 5632], P(None, ('kv', 'tp')), may hold values from -0.125 to 0.125
- second_up: bfloat16 [2048, 5632], P(None, ('kv', 'tp')), may hold values from -0.125 to 0.125
- second_down: bfloat16 [5632, 2048], P(('kv', 'tp')), may hold values from -0.078125 to 0.078125
Outputs:
- mixed_stream: bfloat16 [512, 2048], P('dp', ('kv', 'tp')), parts along dimension 0
- new_state: float32 [512, 8, 64, 128], P(('dp', 'kv'), 'tp'), parts along dimension 0
The draws below stay inside these ranges and needn't reach their ends.
There are 4 independent parts, one for each index of `dp`. The reference program is written for one: setup_inputs(seed, part) draws one part's arguments, and reference() takes and returns one part's arrays. A program takes and returns all parts, laid end to end along the dimension named above; an argument that names none is the same for every part. Nothing has to cross between parts.
All inputs are finite; a program needn't handle non-finite values.
Results may differ from the reference program's by a relative error of at most 0.007.
Values may be sent and summed in bfloat16 or wider, within the bound.
A program may use at most 64 MiB of HBM per device.

```python
import math
import jax
import jax.numpy as jnp
from jax import lax

D = 2048
FF = 5632
HEAD_TOTAL = 8
KEY_CHANNELS = 64
VALUE_DIM = 128
SEQS = 128
N_TP = 2


def draw_stream(key, part):
    first_key = jax.random.fold_in(key, 11)
    second_key = jax.random.fold_in(key, 12)
    columns = jnp.arange(D, dtype=jnp.float32)
    rising = 1.0 + 2.0 * columns / D
    rough = jnp.exp(jax.random.uniform(second_key, (D,), jnp.float32, -0.4, 0.4))
    base = jnp.clip(jax.random.normal(first_key, (SEQS, D), jnp.float32), -4.0, 4.0)
    return (base * rising * rough).astype(jnp.bfloat16)


def block_levels(stream_key, shape, cuts, smallest, largest):
    gain = 1.0
    for position, parts in cuts:
        steps = jax.random.uniform(jax.random.fold_in(jax.random.fold_in(stream_key, 6), position), (parts,), jnp.float32, smallest / len(cuts), largest / len(cuts))
        gain = gain * jnp.repeat(jnp.exp(steps), shape[position] // parts).reshape((-1,) + (1,) * (len(shape) - 1 - position))
    return gain


def bell_draw(stream_key, extent, scale, limit, cuts=(), kind=jnp.bfloat16):
    level = block_levels(stream_key, extent, cuts, -0.22, 0.18) if cuts else 1.0
    array = jax.random.normal(stream_key, extent, jnp.float32) * scale * level
    return jnp.minimum(jnp.maximum(array, -limit), limit).astype(kind)


def setup_inputs(seed: int = 0, part: int = 0) -> dict:
    arg_keys = jax.random.split(jax.random.key(seed), 20)
    part_keys = jax.random.split(jax.random.fold_in(arg_keys[19], part), 20)
    stream = draw_stream(jax.random.fold_in(jax.random.fold_in(arg_keys[19], part), 71), part)
    old_state = bell_draw(part_keys[1], (SEQS, HEAD_TOTAL, KEY_CHANNELS, VALUE_DIM), 1.0, 6.0, ((0, 64), (1, 2)), jnp.float32)
    decay_amounts = jnp.clip(jnp.exp(math.log(1.0) - 5.809143 * jax.random.uniform(part_keys[2], (SEQS, HEAD_TOTAL * KEY_CHANNELS), jnp.float32) ** block_levels(part_keys[2], (SEQS, HEAD_TOTAL * KEY_CHANNELS), ((0, 64), (1, 2)), -0.2, 0.2)), 0.003, 1.0)
    first_gain = jnp.clip(1.0 + 0.18 * jax.random.normal(arg_keys[3], (D,), jnp.float32), 0.1, 1.9)
    first_gate = bell_draw(arg_keys[4], (D, FF), D ** -0.5, 0.125, ((1, 128),))
    first_up = bell_draw(arg_keys[5], (D, FF), D ** -0.5, 0.125, ((1, 128),))
    first_down = bell_draw(arg_keys[6], (FF, D), FF ** -0.5, 0.078125, ((0, 128),))
    mixer_gain = jnp.clip(1.0 + 0.18 * jax.random.normal(arg_keys[7], (D,), jnp.float32), 0.1, 1.9)
    query_weight = bell_draw(arg_keys[8], (D, HEAD_TOTAL * KEY_CHANNELS), D ** -0.5, 0.125, ((0, 64), (1, 2)))
    key_weight = bell_draw(arg_keys[9], (D, HEAD_TOTAL * KEY_CHANNELS), D ** -0.5, 0.125, ((0, 64), (1, 2)))
    decay_weight = bell_draw(arg_keys[10], (D, HEAD_TOTAL * KEY_CHANNELS), (D // 16) ** -0.5, 0.5, ((0, 64), (1, 2)))
    value_weight = bell_draw(arg_keys[11], (D, HEAD_TOTAL * VALUE_DIM), D ** -0.5, 0.125, ((0, 64), (1, 2)))
    output_gate_weight = bell_draw(arg_keys[12], (D, HEAD_TOTAL * VALUE_DIM), D ** -0.5, 0.125, ((0, 64), (1, 2)))
    head_gain = jnp.clip(1.0 + 0.18 * jax.random.normal(arg_keys[13], (HEAD_TOTAL * VALUE_DIM,), jnp.float32), 0.1, 1.9)
    output_weight = bell_draw(arg_keys[14], (HEAD_TOTAL * VALUE_DIM, D), (HEAD_TOTAL * VALUE_DIM) ** -0.5, 0.1875, ((0, 2), (1, 64)))
    second_gain = jnp.clip(1.0 + 0.18 * jax.random.normal(arg_keys[15], (D,), jnp.float32), 0.1, 1.9)
    second_gate = bell_draw(arg_keys[16], (D, FF), D ** -0.5, 0.125, ((1, 128),))
    second_up = bell_draw(arg_keys[17], (D, FF), D ** -0.5, 0.125, ((1, 128),))
    second_down = bell_draw(arg_keys[18], (FF, D), FF ** -0.5, 0.078125, ((0, 128),))
    return {"stream": stream, "old_state": old_state, "decay_amounts": decay_amounts, "first_gain": first_gain, "first_gate": first_gate, "first_up": first_up, "first_down": first_down, "mixer_gain": mixer_gain, "query_weight": query_weight, "key_weight": key_weight, "decay_weight": decay_weight, "value_weight": value_weight, "output_gate_weight": output_gate_weight, "head_gain": head_gain, "output_weight": output_weight, "second_gain": second_gain, "second_gate": second_gate, "second_up": second_up, "second_down": second_down}


EPSILON = 1e-06
GATE_SOFTNESS = 16.0

def row_scale_of(rows):
    wide = rows.astype(jnp.float32)
    return lax.rsqrt(lax.optimization_barrier(jnp.mean(wide * wide, axis=-1, keepdims=True)) + EPSILON)

def half_block(stream, norm_gain, w_gate, w_up, w_down):
    row_scale = row_scale_of(stream)
    scaled = (stream.astype(jnp.float32) * norm_gain).astype(jnp.bfloat16)
    gate_part = jnp.dot(scaled, w_gate, preferred_element_type=jnp.float32) * row_scale
    up_part = jnp.dot(scaled, w_up, preferred_element_type=jnp.float32) * row_scale
    hidden = (jax.nn.silu(gate_part) * up_part).astype(jnp.bfloat16)
    result = stream.astype(jnp.float32) + 0.5 * jnp.dot(hidden, w_down, preferred_element_type=jnp.float32)
    return result.astype(jnp.bfloat16)

def reference(stream, old_state, decay_amounts, first_gain, first_gate, first_up, first_down, mixer_gain, query_weight, key_weight, decay_weight, value_weight, output_gate_weight, head_gain, output_weight, second_gain, second_gate, second_up, second_down):
    middle = half_block(stream, first_gain, first_gate, first_up, first_down)
    row_scale = row_scale_of(middle)
    scaled = (middle.astype(jnp.float32) * mixer_gain).astype(jnp.bfloat16)

    def project(weight_block):
        return jnp.dot(scaled, weight_block, preferred_element_type=jnp.float32) * row_scale
    sequence_count = stream.shape[0]
    query = (project(query_weight) * KEY_CHANNELS ** (-0.5)).reshape(sequence_count, HEAD_TOTAL, KEY_CHANNELS)
    keys = project(key_weight).reshape(sequence_count, HEAD_TOTAL, KEY_CHANNELS)
    gate_logits = project(decay_weight).reshape(sequence_count, HEAD_TOTAL, KEY_CHANNELS)
    values = project(value_weight).reshape(sequence_count, HEAD_TOTAL, VALUE_DIM)
    out_gate = project(output_gate_weight)
    decay_logarithm = jax.nn.log_sigmoid(gate_logits) / GATE_SOFTNESS - decay_amounts.reshape(sequence_count, HEAD_TOTAL, KEY_CHANNELS)
    new_state = jnp.exp(decay_logarithm)[..., None] * old_state + keys[..., None] * values[:, :, None, :]
    readout = jnp.einsum('bhk,bhkv->bhv', query, new_state, precision=lax.Precision.HIGHEST)
    normed = readout * lax.rsqrt(lax.optimization_barrier(jnp.mean(readout * readout, axis=-1, keepdims=True)) + EPSILON)
    mixed_heads = (normed.reshape(sequence_count, HEAD_TOTAL * VALUE_DIM) * head_gain * jax.nn.silu(out_gate)).astype(jnp.bfloat16)
    group_width = HEAD_TOTAL * VALUE_DIM // N_TP
    attention_out = jnp.zeros((sequence_count, D), jnp.float32)
    for group in range(N_TP):
        partial_out = jnp.dot(mixed_heads[:, group * group_width:(group + 1) * group_width], output_weight[group * group_width:(group + 1) * group_width], preferred_element_type=jnp.float32).astype(jnp.bfloat16)
        attention_out = attention_out + lax.optimization_barrier(partial_out).astype(jnp.float32)
    after = (middle.astype(jnp.float32) + attention_out).astype(jnp.bfloat16)
    mixed_stream = half_block(after, second_gain, second_gate, second_up, second_down)
    return (mixed_stream, new_state)
```

```python
import functools

import jax
import jax.numpy as jnp
from jax import lax
from jax.experimental import pallas as pl
from jax.experimental.pallas import tpu as pltpu
from jax.sharding import PartitionSpec as P

EPSILON = 1e-06
GATE_SOFTNESS = 16.0
NY = 4
C = 16
HID = 48
NF = 15
F32 = jnp.float32
BF16 = jnp.bfloat16


def copy_to(src, dst, send, recv, **where):
    return pltpu.make_async_remote_copy(
        src_ref=src,
        dst_ref=dst,
        send_sem=send,
        recv_sem=recv,
        device_id=where,
        device_id_type=pl.DeviceIdType.MESH,
    )


def dot(a, b, ca, cb):
    return lax.dot_general(a, b, (((ca,), (cb,)), ((), ())), preferred_element_type=F32)


def kernel(
    NZ,
    FFL,
    sT,
    old,
    dec,
    g1,
    wg1,
    wu1,
    wd1,
    gm,
    wq,
    wk,
    wz,
    wv,
    wo,
    hg,
    wout,
    g2,
    wg2,
    wu2,
    wd2,
    outT,
    new,
    gat1,
    gat2,
    wgu1,
    wgu2,
    wdt1,
    wdt2,
    s0,
    psend,
    own,
    ptp,
    ysend,
    yrecv,
    accf,
    zsend,
    zrecv,
    pair,
    psnd,
    prcv,
    zs,
    zsb,
    zrb,
    mg,
    mgf,
    pj,
    pjr,
    aft,
    ag_z,
    ag_y,
    ag_t,
    rs_t,
    rs_y,
    rs_z,
    tp_s,
    pr_y,
    pr_z,
    mh_y,
    mh_z,
    fin_s,
):
    kv = lax.axis_index("kv")
    t = lax.axis_index("tp")
    z = kv // NY
    y = kv % NY
    R = 2 * NY * NZ
    D = NZ * NY * 2 * C

    def zpeer(k):
        return lax.rem(z + k, NZ)

    def ypeer(k):
        return lax.rem(y + k, NY)

    def at_z(zz):
        return {"kv": zz * NY + y}

    def at_y(yy):
        return {"kv": z * NY + yy}

    other = {"tp": 1 - t}

    def far_first(i):
        return NZ // 2 + (1 - 2 * lax.rem(i, 2)) * ((i + 1) // 2)

    barrier = pltpu.get_barrier_semaphore()

    def greet_z(i, c):
        pl.semaphore_signal(
            barrier, inc=1, device_id=at_z(zpeer(far_first(i))), device_id_type=pl.DeviceIdType.MESH
        )
        return c

    lax.fori_loop(0, NZ - 1, greet_z, 0)
    for k in range(1, NY):
        pl.semaphore_signal(
            barrier, inc=1, device_id=at_y(ypeer(k)), device_id_type=pl.DeviceIdType.MESH
        )
    pl.semaphore_signal(barrier, inc=1, device_id=other, device_id_type=pl.DeviceIdType.MESH)

    seq = lax.broadcasted_iota(jnp.int32, (R, R), 0)
    lane = lax.broadcasted_iota(jnp.int32, (R, R), 1)
    home = (lane % NZ) * (2 * NY) + (lane // (2 * NZ)) * 2 + (lane // NZ) % 2
    perm = jnp.where(seq == home, 1.0, 0.0).astype(BF16)
    s0[...] = dot(sT[...], perm, 1, 0).astype(BF16)

    def fold(wgu, wg, wu, gain):
        row = gain[...]
        pad = jnp.zeros((HID - FFL, D), F32)
        for part, w in enumerate((wg, wu)):
            scaled = jnp.concatenate([w[...].astype(F32) * row, pad], axis=0)
            wgu[part * HID : (part + 1) * HID, :] = scaled.astype(BF16)

    def turn(wdt, wd):
        width = NY * 2 * C
        for b in range(NZ):
            block = wd[:, b * width : (b + 1) * width].astype(F32)
            block = jnp.concatenate([block, jnp.zeros((128 - FFL, width), F32)], axis=0)
            turned = jnp.transpose(block).astype(BF16).reshape(NY, 2, C, 128)
            for p in range(2):
                for yy in range(NY):
                    wdt[p, yy, b] = turned[yy, p]

    fold(wgu1, wg1, wu1, g1)
    pl.semaphore_wait(barrier, NZ - 1 + NY - 1 + 1)

    sends = []

    def gather(phase, src, gat):
        def go(i, c):
            k = far_first(i)
            copy_to(
                src, gat.at[z, y, t], ag_z.at[phase, 0, k], ag_z.at[phase, 1, k], **at_z(zpeer(k))
            ).start()
            return c

        lax.fori_loop(0, NZ - 1, go, 0)
        gat[z, y, t] = src[...]

        def there(k, c):
            copy_to(
                src, gat.at[z, y, t], ag_z.at[phase, 0, k], ag_z.at[phase, 1, k], **at_z(zpeer(k))
            ).wait_recv()
            return c

        def drained(k, c):
            copy_to(
                src, gat.at[z, y, t], ag_z.at[phase, 0, k], ag_z.at[phase, 1, k], **at_z(zpeer(k))
            ).wait_send()
            return c

        sends.append(lambda: lax.fori_loop(1, NZ, drained, 0))
        return there

    def gather_rest(phase, gat, there):
        lax.fori_loop(1, NZ, there, 0)
        column = gat.at[:, y, t]
        ys = []
        for k in range(1, NY):
            c = copy_to(
                column, column, ag_y.at[phase, 0, k], ag_y.at[phase, 1, k], **at_y(ypeer(k))
            )
            c.start()
            ys.append(c)
        ts = []
        for k in range(NY):
            if k:
                ys[k - 1].wait_recv()
            theirs = gat.at[:, lax.rem(y + NY - k, NY), t]
            c = copy_to(theirs, theirs, ag_t.at[phase, 0, k], ag_t.at[phase, 1, k], **other)
            c.start()
            ts.append(c)
        for c in ts:
            c.wait_recv()
        sends.extend(c.wait_send for c in ys + ts)

    def half(phase, gat, wgu, wdt, s_own):
        rows = gat[...].reshape(D, R)
        acc = dot(wgu[...], rows, 1, 0)
        wide = rows.astype(F32)
        scale = lax.rsqrt(jnp.sum(wide * wide, axis=0, keepdims=True) / D + EPSILON)
        gate = acc[:HID] * scale
        up = acc[HID:] * scale
        hidden = (gate * jax.nn.sigmoid(gate) * up).astype(BF16)
        hidden = jnp.concatenate([hidden, jnp.zeros((128 - HID, R), BF16)], axis=0)
        ts = []
        for k in range(1, NY + 1):
            yy = lax.rem(y + k, NY)
            w = wdt[1 - t, yy].reshape(NZ * C, 128)
            psend[phase, k - 1] = dot(w, hidden, 1, 0).astype(BF16).reshape(NZ, C, R)
            c = copy_to(
                psend.at[phase, k - 1],
                ptp.at[phase, k - 1],
                rs_t.at[phase, 0, k - 1],
                rs_t.at[phase, 1, k - 1],
                **other,
            )
            c.start()
            ts.append(c)
        ys = []
        for k in range(1, NY + 1):
            yy = lax.rem(y + k, NY)
            w = wdt[t, yy].reshape(NZ * C, 128)
            mine = dot(w, hidden, 1, 0).reshape(NZ, C, R)
            ts[k - 1].wait_recv()
            both = mine + ptp[phase, k - 1].astype(F32)
            if k < NY:
                ysend[phase, k - 1] = both.astype(BF16)
                c = copy_to(
                    ysend.at[phase, k - 1],
                    yrecv.at[phase, k - 1],
                    rs_y.at[phase, 0, k - 1],
                    rs_y.at[phase, 1, k - 1],
                    **at_y(yy),
                )
                c.start()
                ys.append(c)
        for c in ys:
            c.wait_recv()
        for k in range(1, NY):
            both = both + yrecv[phase, k - 1].astype(F32)
        accf[phase] = both
        zsend[phase] = both.astype(BF16)

        def zcopy(k):
            zz = zpeer(k)
            return copy_to(
                zsend.at[phase, zz],
                zrecv.at[phase, k],
                rs_z.at[phase, 0, k],
                rs_z.at[phase, 1, k],
                **at_z(zz),
            )

        def go(i, c):
            zcopy(far_first(i)).start()
            return c

        def there(k, c):
            zcopy(k).wait_recv()
            return c

        def drained(k, c):
            zcopy(k).wait_send()
            return c

        lax.fori_loop(0, NZ - 1, go, 0)
        lax.fori_loop(1, NZ, there, 0)
        total = accf[phase, z]
        for k in range(1, NZ):
            total = total + zrecv[phase, k].astype(F32)
        sends.extend(c.wait_send for c in ts + ys)
        sends.append(lambda: lax.fori_loop(1, NZ, drained, 0))
        return (s_own + 0.5 * total).astype(BF16)

    there = gather(0, s0, gat1)
    turn(wdt1, wd1)
    fold(wgu2, wg2, wu2, g2)
    turn(wdt2, wd2)
    eye = lax.broadcasted_iota(jnp.int32, (2 * C, 2 * C), 0) == lax.broadcasted_iota(
        jnp.int32, (2 * C, 2 * C), 1
    )
    gain_col = jnp.sum(
        jnp.where(eye, jnp.broadcast_to(gm[...], (2 * C, 2 * C)), 0.0), axis=1, keepdims=True
    )
    gather_rest(0, gat1, there)
    middle = half(0, gat1, wgu1, wdt1, s0[...].astype(F32))

    pair[t] = middle
    c = copy_to(pair.at[t], pair.at[t], tp_s.at[0], tp_s.at[1], **other)
    c.start()
    c.wait_recv()
    sends.append(c.wait_send)

    wide = pair[...].astype(F32).reshape(2 * C, R)
    turned = jnp.transpose(wide)
    u2 = jnp.transpose(wide * gain_col).astype(BF16)
    f = 0
    for w in (wq, wk, wz, wv, wo):
        part = dot(u2, w[...], 1, 0).astype(BF16)
        for j in range(w.shape[1] // 128):
            psnd[:, f] = part[:, j * 128 : (j + 1) * 128].reshape(NY, 2 * NZ, 128)
            f += 1
    squares = jnp.sum(turned * turned, axis=1, keepdims=True)
    psnd[:, f] = jnp.broadcast_to(squares, (R, 128)).astype(BF16).reshape(NY, 2 * NZ, 128)
    ys = []
    for k in range(1, NY):
        yy = ypeer(k)
        c = copy_to(psnd.at[yy], prcv.at[k - 1], pr_y.at[0, k - 1], pr_y.at[1, k - 1], **at_y(yy))
        c.start()
        ys.append(c)
    for c in ys:
        c.wait_recv()
    sends.extend(c.wait_send for c in ys)
    for f in range(NF):
        chunk = psnd[y, f].astype(F32)
        for k in range(1, NY):
            chunk = chunk + prcv[k - 1, f].astype(F32)
        for s in range(2):
            zs[pl.ds(s * 16 + f, NZ, stride=32), :] = chunk[s * NZ : (s + 1) * NZ]
    for s in range(2):
        zs[pl.ds(s * 16 + NF, NZ, stride=32), :] = jnp.zeros((NZ, 128), F32)
    zsb[...] = zs[...].astype(BF16).reshape(NZ, 32, 128)

    def pcopy(k):
        zz = zpeer(k)
        return copy_to(zsb.at[zz], zrb.at[k], pr_z.at[0, k], pr_z.at[1, k], **at_z(zz))

    def pgo(i, c):
        pcopy(far_first(i)).start()
        return c

    def pthere(k, c):
        pcopy(k).wait_recv()
        return c

    def pdrained(k, c):
        pcopy(k).wait_send()
        return c

    lax.fori_loop(0, NZ - 1, pgo, 0)
    lax.fori_loop(1, NZ, pthere, 0)
    sends.append(lambda: lax.fori_loop(1, NZ, pdrained, 0))
    total = zs[pl.ds(pl.multiple_of(z * 32, 32), 32), :]
    for k in range(1, NZ):
        total = total + zrb[k].astype(F32)

    blocks = []
    columns = []
    for s in range(2):
        b = total[s * 16 : (s + 1) * 16]
        b = b * lax.rsqrt(b[NF - 1 : NF] / D + EPSILON)
        blocks.append(b)
        logits = b[4:6]
        amounts = jnp.concatenate([dec[s : s + 1, 0:128], dec[s : s + 1, 128:256]], axis=0)
        sig = jnp.minimum(logits, 0.0) - jnp.log(1.0 + jnp.exp(-jnp.abs(logits)))
        decay = jnp.exp(sig / GATE_SOFTNESS - amounts)
        columns += [b[0:2] * 0.125, b[2:4], decay]
    columns.append(jnp.zeros((128 - 12, 128), F32))
    cols = jnp.transpose(jnp.concatenate(columns, axis=0))
    rows = []
    for s in range(2):
        for h in range(4):
            lo = (h % 2) * 64
            q, k_, a = (
                cols[lo : lo + 64, s * 6 + 2 * i + h // 2 : s * 6 + 2 * i + h // 2 + 1]
                for i in range(3)
            )
            b = blocks[s]
            state = a * old[s, h] + k_ * b[6 + h : 7 + h]
            new[s, h] = state
            read = jnp.sum(q * state, axis=0, keepdims=True)
            normed = read * lax.rsqrt(jnp.mean(read * read, axis=1, keepdims=True) + EPSILON)
            o = b[10 + h : 11 + h]
            rows.append(normed * hg[h : h + 1] * (o * jax.nn.sigmoid(o)))
    mg[y, z] = jnp.concatenate(rows, axis=0).astype(BF16)

    def mcopy(k):
        own_block = mg.at[y, z]
        return copy_to(own_block, own_block, mh_z.at[0, k], mh_z.at[1, k], **at_z(zpeer(k)))

    def mgo(i, c):
        mcopy(far_first(i)).start()
        return c

    def mthere(k, c):
        mcopy(k).wait_recv()
        return c

    def mdrained(k, c):
        mcopy(k).wait_send()
        return c

    lax.fori_loop(0, NZ - 1, mgo, 0)
    lax.fori_loop(1, NZ, mthere, 0)
    sends.append(lambda: lax.fori_loop(1, NZ, mdrained, 0))
    ys = []
    for k in range(1, NY):
        c = copy_to(mg.at[y], mg.at[y], mh_y.at[0, k], mh_y.at[1, k], **at_y(ypeer(k)))
        c.start()
        ys.append(c)
    for c in ys:
        c.wait_recv()
    sends.extend(c.wait_send for c in ys)
    mgf[...] = mg[...].astype(F32).reshape(NY * NZ * 8, 128)
    heads = []
    for h in range(4):
        pieces = [
            mgf[pl.ds(yy * NZ * 8 + s * 4 + h, NZ, stride=8), :] for yy in range(NY) for s in range(2)
        ]
        heads.append(jnp.concatenate(pieces, axis=0))
    mixed = jnp.concatenate(heads, axis=1).astype(BF16)
    pj[...] = dot(wout[...], mixed, 1, 1).astype(BF16).reshape(2, C, R)
    c = copy_to(pj.at[1 - t], pjr, fin_s.at[0], fin_s.at[1], **other)
    c.start()
    c.wait_recv()
    sends.append(c.wait_send)
    attention = pj[t].astype(F32) + pjr[...].astype(F32)
    after = (middle.astype(F32) + attention).astype(BF16)
    aft[...] = after

    there = gather(1, aft, gat2)
    gather_rest(1, gat2, there)
    result = half(1, gat2, wgu2, wdt2, after.astype(F32))
    outT[...] = dot(result, perm, 1, 1).astype(BF16)
    for wait in sends:
        wait()


def body(
    stream,
    old_state,
    decay_amounts,
    first_gain,
    first_gate,
    first_up,
    first_down,
    mixer_gain,
    query_weight,
    key_weight,
    decay_weight,
    value_weight,
    output_gate_weight,
    head_gain,
    output_weight,
    second_gain,
    second_gate,
    second_up,
    second_down,
):
    NZ = lax.axis_size("kv") // NY
    R = 2 * NY * NZ
    D = NY * NZ * 2 * C
    V = pltpu.VMEM
    S = pltpu.SemaphoreType.DMA
    outT, new = pl.pallas_call(
        functools.partial(kernel, NZ, first_gate.shape[1]),
        out_shape=(
            jax.ShapeDtypeStruct((C, R), BF16),
            jax.ShapeDtypeStruct(old_state.shape, F32),
        ),
        in_specs=[pl.BlockSpec(memory_space=pltpu.VMEM)] * 19,
        out_specs=[pl.BlockSpec(memory_space=pltpu.VMEM)] * 2,
        scratch_shapes=[
            V((NZ, NY, 2, C, R), BF16),
            V((NZ, NY, 2, C, R), BF16),
            V((2 * HID, D), BF16),
            V((2 * HID, D), BF16),
            V((2, NY, NZ, C, 128), BF16),
            V((2, NY, NZ, C, 128), BF16),
            V((C, R), BF16),
            V((2, NY, NZ, C, R), BF16),
            V((8, 128), F32),
            V((2, NY, NZ, C, R), BF16),
            V((2, NY - 1, NZ, C, R), BF16),
            V((2, NY - 1, NZ, C, R), BF16),
            V((2, NZ, C, R), F32),
            V((2, NZ, C, R), BF16),
            V((2, NZ, C, R), BF16),
            V((2, C, R), BF16),
            V((NY, NF, 2 * NZ, 128), BF16),
            V((NY - 1, NF, 2 * NZ, 128), BF16),
            V((NZ * 32, 128), F32),
            V((NZ, 32, 128), BF16),
            V((NZ, 32, 128), BF16),
            V((NY, NZ, 8, 128), BF16),
            V((NY * NZ * 8, 128), F32),
            V((2, C, R), BF16),
            V((C, R), BF16),
            V((C, R), BF16),
            S((2, 2, NZ)),
            S((2, 2, NY)),
            S((2, 2, NY)),
            S((2, 2, NY)),
            S((2, 2, NY)),
            S((2, 2, NZ)),
            S((2,)),
            S((2, NY)),
            S((2, NZ)),
            S((2, NY)),
            S((2, NZ)),
            S((2,)),
        ],
        compiler_params=pltpu.CompilerParams(collective_id=0, has_side_effects=True),
        name="layer",
    )(
        stream.T,
        old_state,
        decay_amounts,
        first_gain.reshape(1, D),
        first_gate.T,
        first_up.T,
        first_down,
        mixer_gain.reshape(1, 2 * C),
        query_weight,
        key_weight,
        decay_weight,
        value_weight,
        output_gate_weight,
        head_gain.reshape(4, 128),
        output_weight.T,
        second_gain.reshape(1, D),
        second_gate.T,
        second_up.T,
        second_down,
    )
    return outT.T, new


def solution(mesh):
    in_specs = (
        P("dp", ("kv", "tp")),
        P(("dp", "kv"), "tp", None, None),
        P(("dp", "kv"), "tp"),
        P(),
        P(None, ("kv", "tp")),
        P(None, ("kv", "tp")),
        P(("kv", "tp"), None),
        P("kv"),
        P("kv", "tp"),
        P("kv", "tp"),
        P("kv", "tp"),
        P("kv", "tp"),
        P("kv", "tp"),
        P("tp"),
        P("tp", "kv"),
        P(),
        P(None, ("kv", "tp")),
        P(None, ("kv", "tp")),
        P(("kv", "tp"), None),
    )
    out_specs = (P("dp", ("kv", "tp")), P(("dp", "kv"), "tp", None, None))
    return jax.shard_map(body, mesh=mesh, in_specs=in_specs, out_specs=out_specs, check_vma=False)
```

```python
import functools

import jax
import jax.numpy as jnp
from jax import lax
from jax.experimental import pallas as pl
from jax.experimental.pallas import tpu as pltpu
from jax.sharding import PartitionSpec as P

EPSILON = 1e-06
GATE_SOFTNESS = 16.0
NY = 4
C = 16
HID = 48
NF = 15
F32 = jnp.float32
BF16 = jnp.bfloat16


def copy_to(src, dst, send, recv, **where):
    return pltpu.make_async_remote_copy(
        src_ref=src,
        dst_ref=dst,
        send_sem=send,
        recv_sem=recv,
        device_id=where,
        device_id_type=pl.DeviceIdType.MESH,
    )


def dot(a, b, ca, cb):
    return lax.dot_general(a, b, (((ca,), (cb,)), ((), ())), preferred_element_type=F32)


def kernel(NZ, FFL, *refs):
    hbm = refs[:19]
    outT, new = refs[19:21]
    local = refs[21:40]
    (
        newv,
        gat1,
        gat2,
        wgu1,
        wgu2,
        wdt1,
        wdt2,
        s0,
        psend,
        ptp,
        ysend,
        yrecv,
        accf,
        zsend,
        zrecv,
        midg,
        wall,
        wsh,
        zs,
        zsb,
        zrb,
        tot,
        ytot,
        mg,
        mgf,
        pj,
        pjr,
        ld,
        ag,
        ag_t,
        rs_t,
        rs_y,
        rs_z,
        md,
        w_y,
        pr_z,
        pr_y,
        mh,
        fin_s,
    ) = refs[40:]
    (
        sT,
        old,
        dec,
        g1,
        wg1,
        wu1,
        wd1,
        gm,
        wq,
        wk,
        wz,
        wv,
        wo,
        hg,
        wout,
        g2,
        wg2,
        wu2,
        wd2,
    ) = local
    kv = lax.axis_index("kv")
    t = lax.axis_index("tp")
    z = kv // NY
    y = kv % NY
    R = 2 * NY * NZ
    D = NZ * NY * 2 * C

    def zpeer(k):
        return lax.rem(z + k, NZ)

    def ypeer(k):
        return lax.rem(y + k, NY)

    def yfrom(k):
        return lax.rem(y + NY - k, NY)

    def at_z(zz):
        return {"kv": zz * NY + y}

    def at_y(yy):
        return {"kv": z * NY + yy}

    other = {"tp": 1 - t}

    def far_first(i):
        return NZ // 2 + (1 - 2 * lax.rem(i, 2)) * ((i + 1) // 2)

    barrier = pltpu.get_barrier_semaphore()

    def greet(**where):
        pl.semaphore_signal(
            barrier, inc=1, device_id=where, device_id_type=pl.DeviceIdType.MESH
        )

    def greet_z(i, c):
        greet(**at_z(zpeer(far_first(i))))
        return c

    lax.fori_loop(0, NZ - 1, greet_z, 0)
    for k in range(1, NY):
        greet(**at_y(ypeer(k)))
        greet(**at_y(ypeer(k)), **other)
    greet(**other)

    def load(i):
        return pltpu.make_async_copy(hbm[i], local[i], ld.at[i])

    for i in (0, 3, 4, 5, 6, 7, 8, 9, 10, 11, 12, 15, 16, 17, 18, 1, 2, 13, 14):
        load(i).start()

    seq = lax.broadcasted_iota(jnp.int32, (R, R), 0)
    lane = lax.broadcasted_iota(jnp.int32, (R, R), 1)
    home = (lane % NZ) * (2 * NY) + (lane // (2 * NZ)) * 2 + (lane // NZ) % 2
    perm = jnp.where(seq == home, 1.0, 0.0).astype(BF16)
    load(0).wait()
    s0[...] = dot(sT[...], perm, 1, 0).astype(BF16)

    def fold(wgu, wg, wu, gain):
        row = gain[...]
        pad = jnp.zeros((HID - FFL, D), F32)
        for part, w in enumerate((wg, wu)):
            scaled = jnp.concatenate([w[...].astype(F32) * row, pad], axis=0)
            wgu[part * HID : (part + 1) * HID, :] = scaled.astype(BF16)

    def turn(wdt, wd):
        width = NY * 2 * C
        for b in range(NZ):
            block = wd[:, b * width : (b + 1) * width].astype(F32)
            block = jnp.concatenate([block, jnp.zeros((128 - FFL, width), F32)], axis=0)
            turned = jnp.transpose(block).astype(BF16).reshape(NY, 2, C, 128)
            for p in range(2):
                for yy in range(NY):
                    wdt[p, yy, b] = turned[yy, p]

    for i in (3, 4, 5):
        load(i).wait()
    fold(wgu1, wg1, wu1, g1)
    load(6).wait()
    turn(wdt1, wd1)
    for i in range(7, 13):
        load(i).wait()
    eye = lax.broadcasted_iota(jnp.int32, (2 * C, 2 * C), 0) == lax.broadcasted_iota(
        jnp.int32, (2 * C, 2 * C), 1
    )
    gain_col = jnp.sum(
        jnp.where(eye, jnp.broadcast_to(gm[...], (2 * C, 2 * C)), 0.0), axis=1, keepdims=True
    )
    f = 0
    for w in (wq, wk, wz, wv, wo):
        scaled = (w[...].astype(F32) * gain_col).astype(BF16)
        for j in range(w.shape[1] // 128):
            wall[f] = scaled[:, j * 128 : (j + 1) * 128]
            f += 1
    for f in range(NF - 1, 4 * NY):
        wall[f] = jnp.zeros((2 * C, 128), BF16)
    pl.semaphore_wait(barrier, NZ - 1 + 2 * (NY - 1) + 1)

    sends = []

    def owe(ref, sem):
        sends.append(copy_to(ref, ref, sem, sem, **other).wait_send)

    def got(ref, sem):
        copy_to(ref, ref, sem, sem, **other).wait_recv()

    G = max(NZ // 4, 1)
    NG = NZ // G
    order = [0] + [(i + 1) // 2 if i % 2 else NG - i // 2 for i in range(1, NG)]

    def gather(slot, most, sem, everything=None, pair_sem=None):
        mine = slot(z, 1, y)

        def send(i, c):
            copy_to(mine, mine, sem.at[0], sem.at[1 + z // G], **at_z(zpeer(far_first(i)))).start()
            return c

        lax.fori_loop(0, NZ - 1, send, 0)
        owe(slot(0, NZ - 1, 0), sem.at[0])

        def finish():
            arrival = 2 + NG
            for i in range(NG):
                q = lax.rem(z // G + order[i], NG)
                n = G if i else G - 1
                if n:
                    got(slot(0, n, 0), sem.at[1 + q])
                group = slot(q * G, G, y)
                for j in (2, 1, 3):
                    copy_to(
                        group,
                        group,
                        sem.at[1 + NG],
                        sem.at[arrival + (j - 1) * NG + i],
                        **at_y(ypeer(j)),
                    ).start()
                if pair_sem is not None:
                    copy_to(group, group, pair_sem.at[0], pair_sem.at[1], **other).start()
            for i in range(NG):
                q = lax.rem(z // G + order[i], NG)
                for j in (1, 3, 2):
                    group = slot(q * G, G, yfrom(j))
                    got(group, sem.at[arrival + (j - 1) * NG + i])
                    if pair_sem is not None:
                        copy_to(group, group, pair_sem.at[0], pair_sem.at[1], **other).start()
            owe(most, sem.at[1 + NG])
            if pair_sem is not None:
                got(everything, pair_sem.at[1])
                owe(everything, pair_sem.at[0])

        return finish

    def half(phase, gat, wgu, wdt, s_own):
        rows = gat[...].reshape(D, R)
        acc = dot(wgu[...], rows, 1, 0)
        wide = rows.astype(F32)
        scale = lax.rsqrt(jnp.sum(wide * wide, axis=0, keepdims=True) / D + EPSILON)
        gate = acc[:HID] * scale
        up = acc[HID:] * scale
        hidden = (gate * jax.nn.sigmoid(gate) * up).astype(BF16)
        hidden = jnp.concatenate([hidden, jnp.zeros((128 - HID, R), BF16)], axis=0)
        ts = []
        for k in range(1, NY + 1):
            yy = lax.rem(y + k, NY)
            w = wdt[1 - t, yy].reshape(NZ * C, 128)
            psend[phase, k - 1] = dot(w, hidden, 1, 0).astype(BF16).reshape(NZ, C, R)
            c = copy_to(
                psend.at[phase, k - 1],
                ptp.at[phase, k - 1],
                rs_t.at[phase, 0],
                rs_t.at[phase, k],
                **other,
            )
            c.start()
            ts.append(c)
        for k in range(1, NY + 1):
            yy = lax.rem(y + k, NY)
            w = wdt[t, yy].reshape(NZ * C, 128)
            mine = dot(w, hidden, 1, 0).reshape(NZ, C, R)
            ts[k - 1].wait_recv()
            both = mine + ptp[phase, k - 1].astype(F32)
            if k < NY:
                ysend[phase, k - 1] = both.astype(BF16)
                c = copy_to(
                    ysend.at[phase, k - 1],
                    yrecv.at[phase, k - 1],
                    rs_y.at[phase, 0],
                    rs_y.at[phase, 1],
                    **at_y(yy),
                )
                c.start()
        owe(psend.at[phase], rs_t.at[phase, 0])
        owe(ysend.at[phase], rs_y.at[phase, 0])
        got(yrecv.at[phase], rs_y.at[phase, 1])
        for k in range(1, NY):
            both = both + yrecv[phase, k - 1].astype(F32)
        accf[phase] = both
        zsend[phase] = both.astype(BF16)
        total = scatter_z(
            zsend.at[phase], zrecv.at[phase], rs_z.at[phase], lambda: accf[phase, z]
        )
        return (s_own + 0.5 * total).astype(BF16)

    def scatter_z(source, landing, sem, mine):
        def send(i, c):
            k = far_first(i)
            zz = zpeer(k)
            copy_to(source.at[zz], landing.at[k], sem.at[0], sem.at[1], **at_z(zz)).start()
            return c

        lax.fori_loop(0, NZ - 1, send, 0)
        owe(landing.at[pl.ds(1, NZ - 1)], sem.at[0])
        total = mine()
        got(landing.at[pl.ds(1, NZ - 1)], sem.at[1])
        for k in range(1, NZ):
            total = total + landing[k].astype(F32)
        return total

    gat1[z, y, t] = s0[...]
    finish = gather(
        lambda zz, n, yy: gat1.at[pl.ds(zz, n), yy, t],
        gat1.at[:, pl.ds(0, NY - 1), t],
        ag.at[0],
        gat1.at[:, :, t],
        ag_t.at[0],
    )
    for k in range(1, NY):
        yy = ypeer(k)
        copy_to(wall.at[pl.ds(4 * yy, 4)], wsh.at[y], w_y.at[0], w_y.at[1], **at_y(yy)).start()
    owe(wall.at[pl.ds(0, 4 * (NY - 1))], w_y.at[0])
    wsh[y] = wall[pl.ds(4 * y, 4)]
    finish()
    for i in (15, 16, 17, 18):
        load(i).wait()
    middle = half(0, gat1, wgu1, wdt1, s0[...].astype(F32))

    here = midg.at[2 * y + t]
    here[...] = middle
    for k in range(NY):
        where = at_y(ypeer(k))
        copy_to(here, here, md.at[0], md.at[1], **where, **other).start()
        if k:
            copy_to(here, here, md.at[0], md.at[1], **where).start()
    most = midg.at[pl.ds(0, 2 * NY - 1)]
    owe(most, md.at[0])
    got(wsh.at[pl.ds(0, NY - 1)], w_y.at[1])
    got(most, md.at[1])

    turned = jnp.transpose(midg[...].astype(F32).reshape(NY * 2 * C, R))
    squares = jnp.sum(turned * turned, axis=1, keepdims=True)
    squares = squares * jnp.where(y == NY - 1, 1.0, 0.0)
    lhs = turned.astype(BF16)
    for c in range(4):
        part = dot(lhs, wsh[:, c].reshape(NY * 2 * C, 128), 1, 0)
        if c == 2:
            part = part + squares
        for yy in range(NY):
            for s in range(2):
                at = (yy * 2 + s) * NZ
                zs[pl.ds(yy * 8 + s * 4 + c, NZ, stride=32), :] = part[at : at + NZ]
    zsb[...] = zs[...].astype(BF16).reshape(NZ, 32, 128)
    total = scatter_z(
        zsb, zrb, pr_z, lambda: zs[pl.ds(pl.multiple_of(z * 32, 32), 32), :]
    )
    tot[...] = total.reshape(NY, 8, 128)
    for k in range(1, NY):
        yy = ypeer(k)
        copy_to(tot.at[yy], ytot.at[y], pr_y.at[0], pr_y.at[1], **at_y(yy)).start()
    owe(tot.at[pl.ds(0, NY - 1)], pr_y.at[0])
    ytot[y] = tot[y]
    for i in (1, 2, 13, 14):
        load(i).wait()
    got(tot.at[pl.ds(0, NY - 1)], pr_y.at[1])

    blocks = []
    columns = []
    for s in range(2):
        b = jnp.concatenate([ytot[yy, s * 4 : (s + 1) * 4] for yy in range(NY)], axis=0)
        b = b * lax.rsqrt(b[NF - 1 : NF] / D + EPSILON)
        blocks.append(b)
        logits = b[4:6]
        amounts = jnp.concatenate([dec[s : s + 1, 0:128], dec[s : s + 1, 128:256]], axis=0)
        sig = jnp.minimum(logits, 0.0) - jnp.log(1.0 + jnp.exp(-jnp.abs(logits)))
        decay = jnp.exp(sig / GATE_SOFTNESS - amounts)
        columns += [b[0:2] * 0.125, b[2:4], decay]
    columns.append(jnp.zeros((128 - 12, 128), F32))
    cols = jnp.transpose(jnp.concatenate(columns, axis=0))
    rows = []
    for s in range(2):
        for h in range(4):
            lo = (h % 2) * 64
            q, k_, a = (
                cols[lo : lo + 64, s * 6 + 2 * i + h // 2 : s * 6 + 2 * i + h // 2 + 1]
                for i in range(3)
            )
            b = blocks[s]
            state = a * old[s, h] + k_ * b[6 + h : 7 + h]
            newv[s, h] = state
            read = jnp.sum(q * state, axis=0, keepdims=True)
            normed = read * lax.rsqrt(jnp.mean(read * read, axis=1, keepdims=True) + EPSILON)
            o = b[10 + h : 11 + h]
            rows.append(normed * hg[h : h + 1] * (o * jax.nn.sigmoid(o)))
    mg[y, z] = jnp.concatenate(rows, axis=0).astype(BF16)

    finish = gather(lambda zz, n, yy: mg.at[yy, pl.ds(zz, n)], mg.at[pl.ds(0, NY - 1)], mh)
    out_copy = pltpu.make_async_copy(newv, new, ld.at[0])
    out_copy.start()
    sends.append(out_copy.wait)
    fold(wgu2, wg2, wu2, g2)
    turn(wdt2, wd2)
    finish()
    mgf[...] = mg[...].astype(F32).reshape(NY * NZ * 8, 128)
    heads = []
    for h in range(4):
        pieces = [
            mgf[pl.ds(yy * NZ * 8 + s * 4 + h, NZ, stride=8), :] for yy in range(NY) for s in range(2)
        ]
        heads.append(jnp.concatenate(pieces, axis=0))
    mixed = jnp.concatenate(heads, axis=1).astype(BF16)
    pj[...] = dot(wout[...], mixed, 1, 1).astype(BF16).reshape(2, C, R)
    c = copy_to(pj.at[1 - t], pjr, fin_s.at[0], fin_s.at[1], **other)
    c.start()
    sends.append(c.wait_send)
    c.wait_recv()
    attention = pj[t].astype(F32) + pjr[...].astype(F32)
    after = (middle.astype(F32) + attention).astype(BF16)

    gat2[z, y, t] = after
    gather(
        lambda zz, n, yy: gat2.at[pl.ds(zz, n), yy, t],
        gat2.at[:, pl.ds(0, NY - 1), t],
        ag.at[1],
        gat2.at[:, :, t],
        ag_t.at[1],
    )()
    result = half(1, gat2, wgu2, wdt2, after.astype(F32))
    outT[...] = dot(result, perm, 1, 1).astype(BF16)
    for wait in sends:
        wait()


def body(
    stream,
    old_state,
    decay_amounts,
    first_gain,
    first_gate,
    first_up,
    first_down,
    mixer_gain,
    query_weight,
    key_weight,
    decay_weight,
    value_weight,
    output_gate_weight,
    head_gain,
    output_weight,
    second_gain,
    second_gate,
    second_up,
    second_down,
):
    NZ = lax.axis_size("kv") // NY
    R = 2 * NY * NZ
    D = NY * NZ * 2 * C
    NG = NZ // max(NZ // 4, 1)
    V = pltpu.VMEM
    S = pltpu.SemaphoreType.DMA
    arrays = (
        stream.T,
        old_state,
        decay_amounts,
        first_gain.reshape(1, D),
        first_gate.T,
        first_up.T,
        first_down,
        mixer_gain.reshape(1, 2 * C),
        query_weight,
        key_weight,
        decay_weight,
        value_weight,
        output_gate_weight,
        head_gain.reshape(4, 128),
        output_weight.T,
        second_gain.reshape(1, D),
        second_gate.T,
        second_up.T,
        second_down,
    )
    outT, new = pl.pallas_call(
        functools.partial(kernel, NZ, first_gate.shape[1]),
        out_shape=(
            jax.ShapeDtypeStruct((C, R), BF16),
            jax.ShapeDtypeStruct(old_state.shape, F32),
        ),
        in_specs=[pl.BlockSpec(memory_space=pl.ANY)] * 19,
        out_specs=[pl.BlockSpec(memory_space=pltpu.VMEM), pl.BlockSpec(memory_space=pl.ANY)],
        scratch_shapes=[V(a.shape, a.dtype) for a in arrays]
        + [
            V(old_state.shape, F32),
            V((NZ, NY, 2, C, R), BF16),
            V((NZ, NY, 2, C, R), BF16),
            V((2 * HID, D), BF16),
            V((2 * HID, D), BF16),
            V((2, NY, NZ, C, 128), BF16),
            V((2, NY, NZ, C, 128), BF16),
            V((C, R), BF16),
            V((2, NY, NZ, C, R), BF16),
            V((2, NY, NZ, C, R), BF16),
            V((2, NY - 1, NZ, C, R), BF16),
            V((2, NY - 1, NZ, C, R), BF16),
            V((2, NZ, C, R), F32),
            V((2, NZ, C, R), BF16),
            V((2, NZ, C, R), BF16),
            V((2 * NY, C, R), BF16),
            V((4 * NY, 2 * C, 128), BF16),
            V((NY, 4, 2 * C, 128), BF16),
            V((NZ * 32, 128), F32),
            V((NZ, 32, 128), BF16),
            V((NZ, 32, 128), BF16),
            V((NY, 8, 128), F32),
            V((NY, 8, 128), F32),
            V((NY, NZ, 8, 128), BF16),
            V((NY * NZ * 8, 128), F32),
            V((2, C, R), BF16),
            V((C, R), BF16),
            S((19,)),
            S((2, 2 + NY * NG)),
            S((2, 2)),
            S((2, 1 + NY)),
            S((2, 2)),
            S((2, 2)),
            S((2,)),
            S((2,)),
            S((2,)),
            S((2,)),
            S((2 + NY * NG,)),
            S((2,)),
        ],
        compiler_params=pltpu.CompilerParams(collective_id=0, has_side_effects=True),
        name="layer",
    )(*arrays)
    return outT.T, new


def solution(mesh):
    in_specs = (
        P("dp", ("kv", "tp")),
        P(("dp", "kv"), "tp", None, None),
        P(("dp", "kv"), "tp"),
        P(),
        P(None, ("kv", "tp")),
        P(None, ("kv", "tp")),
        P(("kv", "tp"), None),
        P("kv"),
        P("kv", "tp"),
        P("kv", "tp"),
        P("kv", "tp"),
        P("kv", "tp"),
        P("kv", "tp"),
        P("tp"),
        P("tp", "kv"),
        P(),
        P(None, ("kv", "tp")),
        P(None, ("kv", "tp")),
        P(("kv", "tp"), None),
    )
    out_specs = (P("dp", ("kv", "tp")), P(("dp", "kv"), "tp", None, None))
    return jax.shard_map(body, mesh=mesh, in_specs=in_specs, out_specs=out_specs, check_vma=False)
```

```python
import functools

import jax
import jax.numpy as jnp
from jax import lax
from jax.experimental import pallas as pl
from jax.experimental.pallas import tpu as pltpu
from jax.sharding import PartitionSpec as P

EPSILON = 1e-06
GATE_SOFTNESS = 16.0
NY = 4
C = 16
HID = 48
NF = 15
F32 = jnp.float32
BF16 = jnp.bfloat16


def copy_to(src, dst, send, recv, **where):
    return pltpu.make_async_remote_copy(
        src_ref=src,
        dst_ref=dst,
        send_sem=send,
        recv_sem=recv,
        device_id=where,
        device_id_type=pl.DeviceIdType.MESH,
    )


def dot(a, b, ca, cb):
    return lax.dot_general(a, b, (((ca,), (cb,)), ((), ())), preferred_element_type=F32)


def kernel(NZ, FFL, *refs):
    hbm = refs[:19]
    outT, new = refs[19:21]
    local = refs[21:40]
    (
        newv,
        gat1,
        gat2,
        wgu1,
        wgu2,
        wdt1,
        wdt2,
        s0,
        psend,
        ptp,
        ysend,
        yrecv,
        accf,
        zsend,
        zrecv,
        midg,
        wall,
        wsh,
        wog,
        trn,
        zs,
        zsb,
        zrb,
        tot,
        ytot,
        mg,
        mgf,
        pj,
        pjr,
        aft,
        ld,
        ag,
        ag_t,
        rs_t,
        rs_y,
        rs_z,
        md,
        w_y,
        wo_y,
        pr_z,
        pr_y,
        mh,
        fin_s,
    ) = refs[40:]
    (
        sT,
        old,
        dec,
        g1,
        wg1,
        wu1,
        wd1,
        gm,
        wq,
        wk,
        wz,
        wv,
        wo,
        hg,
        wout,
        g2,
        wg2,
        wu2,
        wd2,
    ) = local
    kv = lax.axis_index("kv")
    t = lax.axis_index("tp")
    z = kv // NY
    y = kv % NY
    R = 2 * NY * NZ
    D = NZ * NY * 2 * C

    def zpeer(k):
        return lax.rem(z + k, NZ)

    def ypeer(k):
        return lax.rem(y + k, NY)

    def yfrom(k):
        return lax.rem(y + NY - k, NY)

    def at_z(zz):
        return {"kv": zz * NY + y}

    def at_y(yy):
        return {"kv": z * NY + yy}

    other = {"tp": 1 - t}

    def far_first(i):
        return NZ // 2 + (1 - 2 * lax.rem(i, 2)) * ((i + 1) // 2)

    barrier = pltpu.get_barrier_semaphore()

    def greet(**where):
        pl.semaphore_signal(
            barrier, inc=1, device_id=where, device_id_type=pl.DeviceIdType.MESH
        )

    def greet_z(i, c):
        greet(**at_z(zpeer(far_first(i))))
        return c

    lax.fori_loop(0, NZ - 1, greet_z, 0)
    for k in range(1, NY):
        greet(**at_y(ypeer(k)))
        greet(**at_y(ypeer(k)), **other)
    greet(**other)

    def load(i):
        return pltpu.make_async_copy(hbm[i], local[i], ld.at[i])

    for i in (0, 3, 4, 5, 6, 7, 8, 9, 10, 11, 12, 15, 16, 17, 18, 1, 2, 13, 14):
        load(i).start()

    seq = lax.broadcasted_iota(jnp.int32, (R, R), 0)
    lane = lax.broadcasted_iota(jnp.int32, (R, R), 1)
    home = (lane % NZ) * (2 * NY) + (lane // (2 * NZ)) * 2 + (lane // NZ) % 2
    perm = jnp.where(seq == home, 1.0, 0.0).astype(BF16)
    load(0).wait()
    s0[...] = dot(sT[...], perm, 1, 0).astype(BF16)

    def fold(wgu, wg, wu, gain):
        row = gain[...]
        pad = jnp.zeros((HID - FFL, D), F32)
        for part, w in enumerate((wg, wu)):
            scaled = jnp.concatenate([w[...].astype(F32) * row, pad], axis=0)
            wgu[part * HID : (part + 1) * HID, :] = scaled.astype(BF16)
        if wgu.shape[0] > 2 * HID:
            wgu[2 * HID :, :] = jnp.zeros((wgu.shape[0] - 2 * HID, D), BF16)

    def turn(wdt, wd):
        width = NY * 2 * C
        for b in range(NZ):
            block = wd[:, b * width : (b + 1) * width].astype(F32)
            block = jnp.concatenate([block, jnp.zeros((128 - FFL, width), F32)], axis=0)
            turned = jnp.transpose(block).astype(BF16).reshape(NY, 2, C, 128)
            for p in range(2):
                for yy in range(NY):
                    wdt[p, yy, b] = turned[yy, p]

    for i in (3, 4, 5):
        load(i).wait()
    fold(wgu1, wg1, wu1, g1)
    load(6).wait()
    turn(wdt1, wd1)
    for i in range(7, 13):
        load(i).wait()
    eye = lax.broadcasted_iota(jnp.int32, (2 * C, 2 * C), 0) == lax.broadcasted_iota(
        jnp.int32, (2 * C, 2 * C), 1
    )
    gain_col = jnp.sum(
        jnp.where(eye, jnp.broadcast_to(gm[...], (2 * C, 2 * C)), 0.0), axis=1, keepdims=True
    )
    f = 0
    for w in (wq, wk, wz, wv, wo):
        scaled = (w[...].astype(F32) * gain_col).astype(BF16)
        for j in range(w.shape[1] // 128):
            wall[f] = scaled[:, j * 128 : (j + 1) * 128]
            f += 1
    for f in range(NF - 1, 4 * NY):
        wall[f] = jnp.zeros((2 * C, 128), BF16)
    pl.semaphore_wait(barrier, NZ - 1 + 2 * (NY - 1) + 1)

    sends = []

    def owe(ref, sem):
        sends.append(copy_to(ref, ref, sem, sem, **other).wait_send)

    def got(ref, sem):
        copy_to(ref, ref, sem, sem, **other).wait_recv()

    G = max(NZ // 4, 1)
    NG = NZ // G
    order = [0] + [(i + 1) // 2 if i % 2 else NG - i // 2 for i in range(1, NG)]

    def gather(slot, most, sem, everything=None, pair_sem=None):
        mine = slot(z, 1, y)

        def send(i, c):
            copy_to(mine, mine, sem.at[0], sem.at[1 + z // G], **at_z(zpeer(far_first(i)))).start()
            return c

        lax.fori_loop(0, NZ - 1, send, 0)
        owe(slot(0, NZ - 1, 0), sem.at[0])

        def finish():
            arrival = 2 + NG
            for i in range(NG):
                q = lax.rem(z // G + order[i], NG)
                n = G if i else G - 1
                if n:
                    got(slot(0, n, 0), sem.at[1 + q])
                group = slot(q * G, G, y)
                for j in (2, 1, 3):
                    copy_to(
                        group,
                        group,
                        sem.at[1 + NG],
                        sem.at[arrival + (j - 1) * NG + i],
                        **at_y(ypeer(j)),
                    ).start()
                if pair_sem is not None:
                    copy_to(group, group, pair_sem.at[0], pair_sem.at[1], **other).start()
            for i in range(NG):
                q = lax.rem(z // G + order[i], NG)
                for j in (1, 3, 2):
                    group = slot(q * G, G, yfrom(j))
                    got(group, sem.at[arrival + (j - 1) * NG + i])
                    if pair_sem is not None:
                        copy_to(group, group, pair_sem.at[0], pair_sem.at[1], **other).start()
            owe(most, sem.at[1 + NG])
            if pair_sem is not None:
                got(everything, pair_sem.at[1])
                owe(everything, pair_sem.at[0])

        return finish

    def gated(gate, up):
        hidden = (gate * jax.nn.sigmoid(gate) * up).astype(BF16)
        return jnp.concatenate([hidden, jnp.zeros((128 - HID, R), BF16)], axis=0)

    def half(phase, hidden, wdt, meanwhile, residual):
        for k in range(1, NY + 1):
            yy = lax.rem(y + k, NY)
            w = wdt[1 - t, yy].reshape(NZ * C, 128)
            psend[phase, k - 1] = dot(w, hidden, 1, 0).astype(BF16).reshape(NZ, C, R)
            copy_to(
                psend.at[phase, k - 1],
                ptp.at[phase, k - 1],
                rs_t.at[phase, 0],
                rs_t.at[phase, k],
                **other,
            ).start()
        owe(psend.at[phase], rs_t.at[phase, 0])
        far = [(i, pl.ds(lax.rem(z // G + o, NG) * G, G)) for i, o in enumerate(order[::-1])]
        for k in range(1, NY + 1):
            yy = lax.rem(y + k, NY)
            w = wdt[t, yy].reshape(NZ * C, 128)
            mine = dot(w, hidden, 1, 0).reshape(NZ, C, R)
            got(ptp.at[phase, k - 1], rs_t.at[phase, k])
            both = mine + ptp[phase, k - 1].astype(F32)
            if k < NY:
                ysend[phase, k - 1] = both.astype(BF16)
                for i, part in far:
                    copy_to(
                        ysend.at[phase, k - 1, part],
                        yrecv.at[phase, k - 1, part],
                        rs_y.at[phase, 0],
                        rs_y.at[phase, 1 + i],
                        **at_y(yy),
                    ).start()
        accf[phase] = both
        owe(ysend.at[phase], rs_y.at[phase, 0])
        for i, part in far:
            got(yrecv.at[phase, :, part], rs_y.at[phase, 1 + i])
            sums = accf[phase, part]
            for k in range(1, NY):
                sums = sums + yrecv[phase, k - 1, part].astype(F32)
            accf[phase, part] = sums
            zsend[phase, part] = sums.astype(BF16)
            for j in range(G):
                if i < NG - 1:
                    zz = part.start + j
                elif j:
                    zz = part.start + lax.rem(z + j, G)
                else:
                    continue
                copy_to(
                    zsend.at[phase, zz],
                    zrecv.at[phase, lax.rem(zz + NZ - z, NZ)],
                    rs_z.at[phase, 0],
                    rs_z.at[phase, 1],
                    **at_z(zz),
                ).start()
        landed = zrecv.at[phase, pl.ds(1, NZ - 1)]
        owe(landed, rs_z.at[phase, 0])
        meanwhile()
        total = accf[phase, z]
        got(landed, rs_z.at[phase, 1])
        for k in range(1, NZ):
            total = total + zrecv[phase, k].astype(F32)
        return (residual() + 0.5 * total).astype(BF16)

    def scatter_z(source, landing, sem, mine):
        def send(i, c):
            k = far_first(i)
            zz = zpeer(k)
            copy_to(source.at[zz], landing.at[k], sem.at[0], sem.at[1], **at_z(zz)).start()
            return c

        lax.fori_loop(0, NZ - 1, send, 0)
        owe(landing.at[pl.ds(1, NZ - 1)], sem.at[0])
        total = mine()
        got(landing.at[pl.ds(1, NZ - 1)], sem.at[1])
        for k in range(1, NZ):
            total = total + landing[k].astype(F32)
        return total

    gat1[z, y, t] = s0[...]
    finish = gather(
        lambda zz, n, yy: gat1.at[pl.ds(zz, n), yy, t],
        gat1.at[:, pl.ds(0, NY - 1), t],
        ag.at[0],
        gat1.at[:, :, t],
        ag_t.at[0],
    )
    wsh[y] = wall[pl.ds(4 * y, 4)]
    finish()
    all_rows = gat1[...].reshape(D, R)
    acc = dot(wgu1[...], all_rows, 1, 0)
    wide = all_rows.astype(F32)
    scale = lax.rsqrt(jnp.sum(wide * wide, axis=0, keepdims=True) / D + EPSILON)

    def share_weights():
        for k in range(1, NY):
            yy = ypeer(k)
            copy_to(wall.at[pl.ds(4 * yy, 4)], wsh.at[y], w_y.at[0], w_y.at[1], **at_y(yy)).start()
        load(14).wait()
        for k in range(1, NY):
            copy_to(wout, wog.at[y], wo_y.at[0], wo_y.at[1], **at_y(ypeer(k))).start()
        owe(wall.at[pl.ds(0, 4 * (NY - 1))], w_y.at[0])
        owe(wog.at[pl.ds(0, NY - 1)], wo_y.at[0])
        wog[y] = wout[...]

    hidden = gated(acc[:HID] * scale, acc[HID:] * scale)
    middle = half(0, hidden, wdt1, share_weights, lambda: s0[...].astype(F32))

    here = midg.at[2 * y + t]
    here[...] = middle
    for k in range(NY):
        where = at_y(ypeer(k))
        copy_to(here, here, md.at[0], md.at[1], **where, **other).start()
        if k:
            copy_to(here, here, md.at[0], md.at[1], **where).start()
    most = midg.at[pl.ds(0, 2 * NY - 1)]
    owe(most, md.at[0])
    got(wsh.at[pl.ds(0, NY - 1)], w_y.at[1])
    got(most, md.at[1])

    turned = jnp.transpose(midg[...].astype(F32).reshape(NY * 2 * C, R))
    trn[...] = turned.reshape(2 * NY, NZ, 128)
    squares = jnp.sum(turned * turned, axis=1, keepdims=True)
    squares = squares * jnp.where(y == NY - 1, 1.0, 0.0)
    lhs = turned.astype(BF16)
    for c in range(4):
        part = dot(lhs, wsh[:, c].reshape(NY * 2 * C, 128), 1, 0)
        if c == 2:
            part = part + squares
        for yy in range(NY):
            for s in range(2):
                at = (yy * 2 + s) * NZ
                zs[pl.ds(yy * 8 + s * 4 + c, NZ, stride=32), :] = part[at : at + NZ]
    zsb[...] = zs[...].astype(BF16).reshape(NZ, 32, 128)
    total = scatter_z(
        zsb, zrb, pr_z, lambda: zs[pl.ds(pl.multiple_of(z * 32, 32), 32), :]
    )
    tot[...] = total.reshape(NY, 8, 128)
    for k in range(1, NY):
        yy = ypeer(k)
        copy_to(tot.at[yy], ytot.at[y], pr_y.at[0], pr_y.at[1], **at_y(yy)).start()
    owe(tot.at[pl.ds(0, NY - 1)], pr_y.at[0])
    ytot[y] = tot[y]
    for i in (1, 2, 13):
        load(i).wait()
    got(tot.at[pl.ds(0, NY - 1)], pr_y.at[1])

    blocks = []
    columns = []
    for s in range(2):
        b = jnp.concatenate([ytot[yy, s * 4 : (s + 1) * 4] for yy in range(NY)], axis=0)
        b = b * lax.rsqrt(b[NF - 1 : NF] / D + EPSILON)
        blocks.append(b)
        logits = b[4:6]
        amounts = jnp.concatenate([dec[s : s + 1, 0:128], dec[s : s + 1, 128:256]], axis=0)
        sig = jnp.minimum(logits, 0.0) - jnp.log(1.0 + jnp.exp(-jnp.abs(logits)))
        decay = jnp.exp(sig / GATE_SOFTNESS - amounts)
        columns += [b[0:2] * 0.125, b[2:4], decay]
    columns.append(jnp.zeros((128 - 12, 128), F32))
    cols = jnp.transpose(jnp.concatenate(columns, axis=0))
    rows = []
    for s in range(2):
        for h in range(4):
            lo = (h % 2) * 64
            q, k_, a = (
                cols[lo : lo + 64, s * 6 + 2 * i + h // 2 : s * 6 + 2 * i + h // 2 + 1]
                for i in range(3)
            )
            b = blocks[s]
            state = a * old[s, h] + k_ * b[6 + h : 7 + h]
            newv[s, h] = state
            read = jnp.sum(q * state, axis=0, keepdims=True)
            normed = read * lax.rsqrt(jnp.mean(read * read, axis=1, keepdims=True) + EPSILON)
            o = b[10 + h : 11 + h]
            rows.append(normed * hg[h : h + 1] * (o * jax.nn.sigmoid(o)))
    mg[z] = jnp.concatenate(rows, axis=0).astype(BF16)

    def send_heads(i, c):
        zz = zpeer(far_first(i))
        copy_to(mg.at[z], mg.at[z], mh.at[0], mh.at[1], **at_z(zz)).start()
        return c

    lax.fori_loop(0, NZ - 1, send_heads, 0)
    owe(mg.at[pl.ds(0, NZ - 1)], mh.at[0])
    out_copy = pltpu.make_async_copy(newv, new, ld.at[0])
    out_copy.start()
    sends.append(out_copy.wait)
    for i in (15, 16, 17, 18):
        load(i).wait()
    fold(wgu2, wg2, wu2, g2)
    turn(wdt2, wd2)
    got(wog.at[pl.ds(0, NY - 1)], wo_y.at[1])
    got(mg.at[pl.ds(0, NZ - 1)], mh.at[1])
    mgf[...] = mg[...].astype(F32).reshape(NZ * 8, 128)
    heads = []
    for h in range(4):
        pieces = [mgf[pl.ds(s * 4 + h, NZ, stride=8), :] for s in range(2)]
        heads.append(jnp.concatenate(pieces, axis=0))
    mixed = jnp.concatenate(heads, axis=1).astype(BF16)
    product = dot(mixed, wog[...].reshape(NY * 2 * C, 512), 1, 1).astype(BF16)
    pj[...] = product.reshape(2, NZ, NY * 2 * C)
    copy_to(pj.at[1 - t], pjr, fin_s.at[0], fin_s.at[1], **other).start()
    owe(pjr, fin_s.at[0])
    got(pjr, fin_s.at[1])
    attention = pj[t].astype(F32) + pjr[...].astype(F32)

    gat2[z, y, t] = (trn[2 * y + t] + attention).astype(BF16)
    gather(
        lambda zz, n, yy: gat2.at[pl.ds(zz, n), yy, t],
        gat2.at[:, pl.ds(0, NY - 1), t],
        ag.at[1],
        gat2.at[:, :, t],
        ag_t.at[1],
    )()
    all_rows = jnp.concatenate([gat2[i].reshape(R, NY * 2 * C) for i in range(NZ)], axis=1)
    acc = dot(all_rows, wgu2[...], 1, 1)
    wide = all_rows.astype(F32)
    scale = lax.rsqrt(jnp.sum(wide * wide, axis=1, keepdims=True) / D + EPSILON)
    acc = jnp.transpose(acc * scale)

    def own_columns():
        block = gat2[z].astype(F32).reshape(R, NY * 2 * C)
        aft[...] = jnp.transpose(block).reshape(2 * NY, C, R)

    hidden = gated(acc[:HID], acc[HID : 2 * HID])
    result = half(1, hidden, wdt2, own_columns, lambda: aft[2 * y + t])
    outT[...] = dot(result, perm, 1, 1).astype(BF16)
    for wait in sends:
        wait()


def body(
    stream,
    old_state,
    decay_amounts,
    first_gain,
    first_gate,
    first_up,
    first_down,
    mixer_gain,
    query_weight,
    key_weight,
    decay_weight,
    value_weight,
    output_gate_weight,
    head_gain,
    output_weight,
    second_gain,
    second_gate,
    second_up,
    second_down,
):
    NZ = lax.axis_size("kv") // NY
    R = 2 * NY * NZ
    D = NY * NZ * 2 * C
    NG = NZ // max(NZ // 4, 1)
    V = pltpu.VMEM
    S = pltpu.SemaphoreType.DMA
    arrays = (
        stream.T,
        old_state,
        decay_amounts,
        first_gain.reshape(1, D),
        first_gate.T,
        first_up.T,
        first_down,
        mixer_gain.reshape(1, 2 * C),
        query_weight,
        key_weight,
        decay_weight,
        value_weight,
        output_gate_weight,
        head_gain.reshape(4, 128),
        output_weight.T,
        second_gain.reshape(1, D),
        second_gate.T,
        second_up.T,
        second_down,
    )
    outT, new = pl.pallas_call(
        functools.partial(kernel, NZ, first_gate.shape[1]),
        out_shape=(
            jax.ShapeDtypeStruct((C, R), BF16),
            jax.ShapeDtypeStruct(old_state.shape, F32),
        ),
        in_specs=[pl.BlockSpec(memory_space=pl.ANY)] * 19,
        out_specs=[pl.BlockSpec(memory_space=pltpu.VMEM), pl.BlockSpec(memory_space=pl.ANY)],
        scratch_shapes=[V(a.shape, a.dtype) for a in arrays]
        + [
            V(old_state.shape, F32),
            V((NZ, NY, 2, C, R), BF16),
            V((NZ, NY, 2, NZ, NY * 2 * C), BF16),
            V((2 * HID, D), BF16),
            V((128, D), BF16),
            V((2, NY, NZ, C, 128), BF16),
            V((2, NY, NZ, C, 128), BF16),
            V((C, R), BF16),
            V((2, NY, NZ, C, R), BF16),
            V((2, NY, NZ, C, R), BF16),
            V((2, NY - 1, NZ, C, R), BF16),
            V((2, NY - 1, NZ, C, R), BF16),
            V((2, NZ, C, R), F32),
            V((2, NZ, C, R), BF16),
            V((2, NZ, C, R), BF16),
            V((2 * NY, C, R), BF16),
            V((4 * NY, 2 * C, 128), BF16),
            V((NY, 4, 2 * C, 128), BF16),
            V((NY, 2 * C, 512), BF16),
            V((2 * NY, NZ, 128), F32),
            V((NZ * 32, 128), F32),
            V((NZ, 32, 128), BF16),
            V((NZ, 32, 128), BF16),
            V((NY, 8, 128), F32),
            V((NY, 8, 128), F32),
            V((NZ, 8, 128), BF16),
            V((NZ * 8, 128), F32),
            V((2, NZ, NY * 2 * C), BF16),
            V((NZ, NY * 2 * C), BF16),
            V((2 * NY, C, R), F32),
            S((19,)),
            S((2, 2 + NY * NG)),
            S((2, 2)),
            S((2, 1 + NY)),
            S((2, 1 + NG)),
            S((2, 2)),
            S((2,)),
            S((2,)),
            S((2,)),
            S((2,)),
            S((2,)),
            S((2,)),
            S((2,)),
        ],
        compiler_params=pltpu.CompilerParams(collective_id=0, has_side_effects=True),
        name="layer",
    )(*arrays)
    return outT.T, new


def solution(mesh):
    in_specs = (
        P("dp", ("kv", "tp")),
        P(("dp", "kv"), "tp", None, None),
        P(("dp", "kv"), "tp"),
        P(),
        P(None, ("kv", "tp")),
        P(None, ("kv", "tp")),
        P(("kv", "tp"), None),
        P("kv"),
        P("kv", "tp"),
        P("kv", "tp"),
        P("kv", "tp"),
        P("kv", "tp"),
        P("kv", "tp"),
        P("tp"),
        P("tp", "kv"),
        P(),
        P(None, ("kv", "tp")),
        P(None, ("kv", "tp")),
        P(("kv", "tp"), None),
    )
    out_specs = (P("dp", ("kv", "tp")), P(("dp", "kv"), "tp", None, None))
    return jax.shard_map(body, mesh=mesh, in_specs=in_specs, out_specs=out_specs, check_vma=False)
```

```python
import functools

import jax
import jax.numpy as jnp
from jax import lax
from jax.experimental import pallas as pl
from jax.experimental.pallas import tpu as pltpu
from jax.sharding import PartitionSpec as P

EPSILON = 1e-06
GATE_SOFTNESS = 16.0
NY = 4
C = 16
HID = 48
NF = 15
F32 = jnp.float32
BF16 = jnp.bfloat16


def copy_to(src, dst, send, recv, **where):
    return pltpu.make_async_remote_copy(
        src_ref=src,
        dst_ref=dst,
        send_sem=send,
        recv_sem=recv,
        device_id=where,
        device_id_type=pl.DeviceIdType.MESH,
    )


def dot(a, b, ca, cb):
    return lax.dot_general(a, b, (((ca,), (cb,)), ((), ())), preferred_element_type=F32)


def kernel(NZ, FFL, *refs):
    hbm = refs[:19]
    outT, new = refs[19:21]
    local = refs[21:40]
    (
        newv,
        gat1,
        gat2,
        wgu1,
        wgu2,
        wdt1,
        wdt2,
        s0,
        psend,
        ptp,
        ysend,
        yrecv,
        accf,
        zsend,
        zrecv,
        midg,
        wall,
        wsh,
        wog,
        trn,
        zs,
        zsb,
        zrb,
        ytot,
        mg,
        mgf,
        pj,
        pjr,
        aft,
        ld,
        ag,
        ag_t,
        rs_t,
        rs_y,
        rs_z,
        md,
        w_y,
        wo_y,
        pr_z,
        mh,
        fin_s,
    ) = refs[40:]
    (
        sT,
        old,
        dec,
        g1,
        wg1,
        wu1,
        wd1,
        gm,
        wq,
        wk,
        wz,
        wv,
        wo,
        hg,
        wout,
        g2,
        wg2,
        wu2,
        wd2,
    ) = local
    kv = lax.axis_index("kv")
    t = lax.axis_index("tp")
    z = kv // NY
    y = kv % NY
    R = 2 * NY * NZ
    D = NZ * NY * 2 * C

    def zpeer(k):
        return lax.rem(z + k, NZ)

    def ypeer(k):
        return lax.rem(y + k, NY)

    def yfrom(k):
        return lax.rem(y + NY - k, NY)

    def at_z(zz):
        return {"kv": zz * NY + y}

    def at_y(yy):
        return {"kv": z * NY + yy}

    other = {"tp": 1 - t}

    def far_first(i):
        return NZ // 2 + (1 - 2 * lax.rem(i, 2)) * ((i + 1) // 2)

    barrier = pltpu.get_barrier_semaphore()

    def greet(**where):
        pl.semaphore_signal(
            barrier, inc=1, device_id=where, device_id_type=pl.DeviceIdType.MESH
        )

    def greet_z(i, c):
        greet(**at_z(zpeer(far_first(i))))
        return c

    lax.fori_loop(0, NZ - 1, greet_z, 0)
    for k in range(1, NY):
        greet(**at_y(ypeer(k)))
        greet(**at_y(ypeer(k)), **other)
    greet(**other)

    def load(i):
        return pltpu.make_async_copy(hbm[i], local[i], ld.at[i])

    for i in (0, 3, 4, 5, 6, 7, 8, 9, 10, 11, 12, 15, 16, 17, 18, 1, 2, 13, 14):
        load(i).start()

    seq = lax.broadcasted_iota(jnp.int32, (R, R), 0)
    lane = lax.broadcasted_iota(jnp.int32, (R, R), 1)
    home = (lane % NZ) * (2 * NY) + (lane // (2 * NZ)) * 2 + (lane // NZ) % 2
    perm = jnp.where(seq == home, 1.0, 0.0).astype(BF16)
    load(0).wait()
    s0[...] = dot(sT[...], perm, 1, 0).astype(BF16)

    def fold(wgu, wg, wu, gain):
        row = gain[...]
        pad = jnp.zeros((HID - FFL, D), F32)
        for part, w in enumerate((wg, wu)):
            scaled = jnp.concatenate([w[...].astype(F32) * row, pad], axis=0)
            wgu[part * HID : (part + 1) * HID, :] = scaled.astype(BF16)
        if wgu.shape[0] > 2 * HID:
            wgu[2 * HID :, :] = jnp.zeros((wgu.shape[0] - 2 * HID, D), BF16)

    def turn(wdt, wd):
        width = NY * 2 * C
        for b in range(NZ):
            block = wd[:, b * width : (b + 1) * width].astype(F32)
            block = jnp.concatenate([block, jnp.zeros((128 - FFL, width), F32)], axis=0)
            turned = jnp.transpose(block).astype(BF16).reshape(NY, 2, C, 128)
            for p in range(2):
                for yy in range(NY):
                    wdt[p, yy, b] = turned[yy, p]

    for i in (3, 4, 5):
        load(i).wait()
    fold(wgu1, wg1, wu1, g1)
    load(6).wait()
    turn(wdt1, wd1)
    for i in range(7, 13):
        load(i).wait()
    eye = lax.broadcasted_iota(jnp.int32, (2 * C, 2 * C), 0) == lax.broadcasted_iota(
        jnp.int32, (2 * C, 2 * C), 1
    )
    gain_col = jnp.sum(
        jnp.where(eye, jnp.broadcast_to(gm[...], (2 * C, 2 * C)), 0.0), axis=1, keepdims=True
    )
    f = 0
    for w in (wq, wk, wz, wv, wo):
        scaled = (w[...].astype(F32) * gain_col).astype(BF16)
        for j in range(w.shape[1] // 128):
            wall[f] = scaled[:, j * 128 : (j + 1) * 128]
            f += 1
    for f in range(NF - 1, 4 * NY):
        wall[f] = jnp.zeros((2 * C, 128), BF16)
    pl.semaphore_wait(barrier, NZ - 1 + 2 * (NY - 1) + 1)

    sends = []

    def owe(ref, sem):
        sends.append(copy_to(ref, ref, sem, sem, **other).wait_send)

    def got(ref, sem):
        copy_to(ref, ref, sem, sem, **other).wait_recv()

    G = max(NZ // 4, 1)
    NG = NZ // G
    order = [0] + [(i + 1) // 2 if i % 2 else NG - i // 2 for i in range(1, NG)]

    def gather(slot, most, sem, everything=None, pair_sem=None):
        mine = slot(z, 1, y)

        def send(i, c):
            copy_to(mine, mine, sem.at[0], sem.at[1 + z // G], **at_z(zpeer(far_first(i)))).start()
            return c

        lax.fori_loop(0, NZ - 1, send, 0)
        owe(slot(0, NZ - 1, 0), sem.at[0])

        def finish():
            arrival = 2 + NG
            for i in range(NG):
                q = lax.rem(z // G + order[i], NG)
                n = G if i else G - 1
                if n:
                    got(slot(0, n, 0), sem.at[1 + q])
                group = slot(q * G, G, y)
                for j in (2, 1, 3):
                    copy_to(
                        group,
                        group,
                        sem.at[1 + NG],
                        sem.at[arrival + (j - 1) * NG + i],
                        **at_y(ypeer(j)),
                    ).start()
                if pair_sem is not None:
                    copy_to(group, group, pair_sem.at[0], pair_sem.at[1], **other).start()
            for i in range(NG):
                q = lax.rem(z // G + order[i], NG)
                for j in (1, 3, 2):
                    group = slot(q * G, G, yfrom(j))
                    got(group, sem.at[arrival + (j - 1) * NG + i])
                    if pair_sem is not None:
                        copy_to(group, group, pair_sem.at[0], pair_sem.at[1], **other).start()
            owe(most, sem.at[1 + NG])
            if pair_sem is not None:
                got(everything, pair_sem.at[1])
                owe(everything, pair_sem.at[0])

        return finish

    def gated(gate, up):
        hidden = (gate * jax.nn.sigmoid(gate) * up).astype(BF16)
        return jnp.concatenate([hidden, jnp.zeros((128 - HID, R), BF16)], axis=0)

    def half(phase, hidden, wdt, meanwhile, residual):
        for k in range(1, NY + 1):
            yy = lax.rem(y + k, NY)
            w = wdt[1 - t, yy].reshape(NZ * C, 128)
            psend[phase, k - 1] = dot(w, hidden, 1, 0).astype(BF16).reshape(NZ, C, R)
            copy_to(
                psend.at[phase, k - 1],
                ptp.at[phase, k - 1],
                rs_t.at[phase, 0],
                rs_t.at[phase, k],
                **other,
            ).start()
        owe(psend.at[phase], rs_t.at[phase, 0])
        far = [(i, pl.ds(lax.rem(z // G + o, NG) * G, G)) for i, o in enumerate(order[::-1])]
        for k in range(1, NY + 1):
            yy = lax.rem(y + k, NY)
            w = wdt[t, yy].reshape(NZ * C, 128)
            mine = dot(w, hidden, 1, 0).reshape(NZ, C, R)
            got(ptp.at[phase, k - 1], rs_t.at[phase, k])
            both = mine + ptp[phase, k - 1].astype(F32)
            if k < NY:
                ysend[phase, k - 1] = both.astype(BF16)
                for i, part in far:
                    copy_to(
                        ysend.at[phase, k - 1, part],
                        yrecv.at[phase, k - 1, part],
                        rs_y.at[phase, 0],
                        rs_y.at[phase, 1 + i],
                        **at_y(yy),
                    ).start()
        accf[phase] = both
        owe(ysend.at[phase], rs_y.at[phase, 0])
        for i, part in far:
            got(yrecv.at[phase, :, part], rs_y.at[phase, 1 + i])
            sums = accf[phase, part]
            for k in range(1, NY):
                sums = sums + yrecv[phase, k - 1, part].astype(F32)
            accf[phase, part] = sums
            zsend[phase, part] = sums.astype(BF16)
            for j in range(G):
                if i < NG - 1:
                    zz = part.start + j
                elif j:
                    zz = part.start + lax.rem(z + j, G)
                else:
                    continue
                copy_to(
                    zsend.at[phase, zz],
                    zrecv.at[phase, lax.rem(zz + NZ - z, NZ)],
                    rs_z.at[phase, 0],
                    rs_z.at[phase, 1],
                    **at_z(zz),
                ).start()
        landed = zrecv.at[phase, pl.ds(1, NZ - 1)]
        owe(landed, rs_z.at[phase, 0])
        meanwhile()
        total = accf[phase, z]
        got(landed, rs_z.at[phase, 1])
        for k in range(1, NZ):
            total = total + zrecv[phase, k].astype(F32)
        return (residual() + 0.5 * total).astype(BF16)

    gat1[z, y, t] = s0[...]
    finish = gather(
        lambda zz, n, yy: gat1.at[pl.ds(zz, n), yy, t],
        gat1.at[:, pl.ds(0, NY - 1), t],
        ag.at[0],
        gat1.at[:, :, t],
        ag_t.at[0],
    )
    wsh[y] = wall[pl.ds(4 * y, 4)]
    finish()
    all_rows = gat1[...].reshape(D, R)
    acc = dot(wgu1[...], all_rows, 1, 0)
    wide = all_rows.astype(F32)
    scale = lax.rsqrt(jnp.sum(wide * wide, axis=0, keepdims=True) / D + EPSILON)

    def share_weights():
        for k in range(1, NY):
            yy = ypeer(k)
            copy_to(wall.at[pl.ds(4 * yy, 4)], wsh.at[y], w_y.at[0], w_y.at[1], **at_y(yy)).start()
        load(14).wait()
        for k in range(1, NY):
            copy_to(wout, wog.at[y], wo_y.at[0], wo_y.at[1], **at_y(ypeer(k))).start()
        owe(wall.at[pl.ds(0, 4 * (NY - 1))], w_y.at[0])
        owe(wog.at[pl.ds(0, NY - 1)], wo_y.at[0])
        wog[y] = wout[...]

    hidden = gated(acc[:HID] * scale, acc[HID:] * scale)
    middle = half(0, hidden, wdt1, share_weights, lambda: s0[...].astype(F32))

    here = midg.at[2 * y + t]
    here[...] = middle
    for k in range(NY):
        where = at_y(ypeer(k))
        copy_to(here, here, md.at[0], md.at[1], **where, **other).start()
        if k:
            copy_to(here, here, md.at[0], md.at[1], **where).start()
    most = midg.at[pl.ds(0, 2 * NY - 1)]
    owe(most, md.at[0])
    got(wsh.at[pl.ds(0, NY - 1)], w_y.at[1])
    got(most, md.at[1])

    turned = jnp.transpose(midg[...].astype(F32).reshape(NY * 2 * C, R))
    trn[...] = turned.reshape(2 * NY, NZ, 128)
    squares = jnp.sum(turned * turned, axis=1, keepdims=True)
    squares = squares * jnp.where(y == NY - 1, 1.0, 0.0)
    lhs = turned.astype(BF16)
    for c in range(4):
        part = dot(lhs, wsh[:, c].reshape(NY * 2 * C, 128), 1, 0)
        if c == 2:
            part = part + squares
        for yy in range(NY):
            for s in range(2):
                at = (yy * 2 + s) * NZ
                zs[pl.ds(yy * 8 + s * 4 + c, NZ, stride=32), :] = part[at : at + NZ]
    zsb[...] = zs[...].astype(BF16).reshape(NZ, NY, 8, 128)

    def send_sums(i, c):
        k = far_first(i)
        zz = zpeer(k)
        for j in (2, 1, 3, 0):
            yy = ypeer(j)
            there = {"kv": zz * NY + yy}
            copy_to(zsb.at[zz, yy], zrb.at[k * NY + y], pr_z.at[0], pr_z.at[1], **there).start()
        return c

    lax.fori_loop(0, NZ - 1, send_sums, 0)
    for j in (2, 1, 3):
        yy = ypeer(j)
        copy_to(zsb.at[z, yy], zrb.at[y], pr_z.at[0], pr_z.at[1], **at_y(yy)).start()
    zrb[y] = zsb[z, y]
    landed = zrb.at[pl.ds(0, NZ * NY - 1)]
    owe(landed, pr_z.at[0])
    for i in (1, 2, 13):
        load(i).wait()
    got(landed, pr_z.at[1])
    for yy in range(NY):
        total = zrb[yy].astype(F32)
        for k in range(1, NZ):
            total = total + zrb[k * NY + yy].astype(F32)
        ytot[yy] = total

    blocks = []
    columns = []
    for s in range(2):
        b = jnp.concatenate([ytot[yy, s * 4 : (s + 1) * 4] for yy in range(NY)], axis=0)
        b = b * lax.rsqrt(b[NF - 1 : NF] / D + EPSILON)
        blocks.append(b)
        logits = b[4:6]
        amounts = jnp.concatenate([dec[s : s + 1, 0:128], dec[s : s + 1, 128:256]], axis=0)
        sig = jnp.minimum(logits, 0.0) - jnp.log(1.0 + jnp.exp(-jnp.abs(logits)))
        decay = jnp.exp(sig / GATE_SOFTNESS - amounts)
        columns += [b[0:2] * 0.125, b[2:4], decay]
    columns.append(jnp.zeros((128 - 12, 128), F32))
    cols = jnp.transpose(jnp.concatenate(columns, axis=0))
    rows = []
    for s in range(2):
        for h in range(4):
            lo = (h % 2) * 64
            q, k_, a = (
                cols[lo : lo + 64, s * 6 + 2 * i + h // 2 : s * 6 + 2 * i + h // 2 + 1]
                for i in range(3)
            )
            b = blocks[s]
            state = a * old[s, h] + k_ * b[6 + h : 7 + h]
            newv[s, h] = state
            read = jnp.sum(q * state, axis=0, keepdims=True)
            normed = read * lax.rsqrt(jnp.mean(read * read, axis=1, keepdims=True) + EPSILON)
            o = b[10 + h : 11 + h]
            rows.append(normed * hg[h : h + 1] * (o * jax.nn.sigmoid(o)))
    mg[z] = jnp.concatenate(rows, axis=0).astype(BF16)

    def send_heads(i, c):
        zz = zpeer(far_first(i))
        copy_to(mg.at[z], mg.at[z], mh.at[0], mh.at[1], **at_z(zz)).start()
        return c

    lax.fori_loop(0, NZ - 1, send_heads, 0)
    owe(mg.at[pl.ds(0, NZ - 1)], mh.at[0])
    out_copy = pltpu.make_async_copy(newv, new, ld.at[0])
    out_copy.start()
    sends.append(out_copy.wait)
    for i in (15, 16, 17, 18):
        load(i).wait()
    fold(wgu2, wg2, wu2, g2)
    turn(wdt2, wd2)
    got(wog.at[pl.ds(0, NY - 1)], wo_y.at[1])
    got(mg.at[pl.ds(0, NZ - 1)], mh.at[1])
    mgf[...] = mg[...].astype(F32).reshape(NZ * 8, 128)
    heads = []
    for h in range(4):
        pieces = [mgf[pl.ds(s * 4 + h, NZ, stride=8), :] for s in range(2)]
        heads.append(jnp.concatenate(pieces, axis=0))
    mixed = jnp.concatenate(heads, axis=1).astype(BF16)
    product = dot(mixed, wog[...].reshape(NY * 2 * C, 512), 1, 1).astype(BF16)
    pj[...] = product.reshape(2, NZ, NY * 2 * C)
    copy_to(pj.at[1 - t], pjr, fin_s.at[0], fin_s.at[1], **other).start()
    owe(pjr, fin_s.at[0])
    got(pjr, fin_s.at[1])
    attention = pj[t].astype(F32) + pjr[...].astype(F32)

    gat2[z, y, t] = (trn[2 * y + t] + attention).astype(BF16)
    gather(
        lambda zz, n, yy: gat2.at[pl.ds(zz, n), yy, t],
        gat2.at[:, pl.ds(0, NY - 1), t],
        ag.at[1],
        gat2.at[:, :, t],
        ag_t.at[1],
    )()
    all_rows = jnp.concatenate([gat2[i].reshape(R, NY * 2 * C) for i in range(NZ)], axis=1)
    acc = dot(all_rows, wgu2[...], 1, 1)
    wide = all_rows.astype(F32)
    scale = lax.rsqrt(jnp.sum(wide * wide, axis=1, keepdims=True) / D + EPSILON)
    acc = jnp.transpose(acc * scale)

    def own_columns():
        block = gat2[z].astype(F32).reshape(R, NY * 2 * C)
        aft[...] = jnp.transpose(block).reshape(2 * NY, C, R)

    hidden = gated(acc[:HID], acc[HID : 2 * HID])
    result = half(1, hidden, wdt2, own_columns, lambda: aft[2 * y + t])
    outT[...] = dot(result, perm, 1, 1).astype(BF16)
    for wait in sends:
        wait()


def write_out(outT, new, outT_ref, new_ref, o_v, n_v, sem):
    parts = new.shape[0]
    moves = [(outT, o_v, outT_ref)] + [(new.at[i], n_v.at[i], new_ref.at[i]) for i in range(parts)]
    ins = [pltpu.make_async_copy(a, v, sem.at[0, i]) for i, (a, v, _) in enumerate(moves)]
    outs = [pltpu.make_async_copy(v, b, sem.at[1, i]) for i, (_, v, b) in enumerate(moves)]
    for c in ins:
        c.start()
    for a, b in zip(ins, outs):
        a.wait()
        b.start()
    for c in outs:
        c.wait()


def body(
    stream,
    old_state,
    decay_amounts,
    first_gain,
    first_gate,
    first_up,
    first_down,
    mixer_gain,
    query_weight,
    key_weight,
    decay_weight,
    value_weight,
    output_gate_weight,
    head_gain,
    output_weight,
    second_gain,
    second_gate,
    second_up,
    second_down,
):
    NZ = lax.axis_size("kv") // NY
    R = 2 * NY * NZ
    D = NY * NZ * 2 * C
    NG = NZ // max(NZ // 4, 1)
    V = pltpu.VMEM
    S = pltpu.SemaphoreType.DMA
    arrays = (
        stream.T,
        old_state,
        decay_amounts,
        first_gain.reshape(1, D),
        first_gate.T,
        first_up.T,
        first_down,
        mixer_gain.reshape(1, 2 * C),
        query_weight,
        key_weight,
        decay_weight,
        value_weight,
        output_gate_weight,
        head_gain.reshape(4, 128),
        output_weight.T,
        second_gain.reshape(1, D),
        second_gate.T,
        second_up.T,
        second_down,
    )
    outT, new = pl.pallas_call(
        functools.partial(kernel, NZ, first_gate.shape[1]),
        out_shape=(
            jax.ShapeDtypeStruct((C, R), BF16),
            jax.ShapeDtypeStruct(old_state.shape, F32),
        ),
        in_specs=[pl.BlockSpec(memory_space=pl.ANY)] * 19,
        out_specs=[pl.BlockSpec(memory_space=pltpu.VMEM), pl.BlockSpec(memory_space=pl.ANY)],
        scratch_shapes=[V(a.shape, a.dtype) for a in arrays]
        + [
            V(old_state.shape, F32),
            V((NZ, NY, 2, C, R), BF16),
            V((NZ, NY, 2, NZ, NY * 2 * C), BF16),
            V((2 * HID, D), BF16),
            V((128, D), BF16),
            V((2, NY, NZ, C, 128), BF16),
            V((2, NY, NZ, C, 128), BF16),
            V((C, R), BF16),
            V((2, NY, NZ, C, R), BF16),
            V((2, NY, NZ, C, R), BF16),
            V((2, NY - 1, NZ, C, R), BF16),
            V((2, NY - 1, NZ, C, R), BF16),
            V((2, NZ, C, R), F32),
            V((2, NZ, C, R), BF16),
            V((2, NZ, C, R), BF16),
            V((2 * NY, C, R), BF16),
            V((4 * NY, 2 * C, 128), BF16),
            V((NY, 4, 2 * C, 128), BF16),
            V((NY, 2 * C, 512), BF16),
            V((2 * NY, NZ, 128), F32),
            V((NZ * 32, 128), F32),
            V((NZ, NY, 8, 128), BF16),
            V((NZ * NY, 8, 128), BF16),
            V((NY, 8, 128), F32),
            V((NZ, 8, 128), BF16),
            V((NZ * 8, 128), F32),
            V((2, NZ, NY * 2 * C), BF16),
            V((NZ, NY * 2 * C), BF16),
            V((2 * NY, C, R), F32),
            S((19,)),
            S((2, 2 + NY * NG)),
            S((2, 2)),
            S((2, 1 + NY)),
            S((2, 1 + NG)),
            S((2, 2)),
            S((2,)),
            S((2,)),
            S((2,)),
            S((2,)),
            S((2,)),
            S((2,)),
        ],
        compiler_params=pltpu.CompilerParams(collective_id=0, has_side_effects=True),
        name="layer",
    )(*arrays)
    outT, new = pl.pallas_call(
        write_out,
        out_shape=(
            jax.ShapeDtypeStruct(outT.shape, BF16),
            jax.ShapeDtypeStruct(new.shape, F32),
        ),
        in_specs=[pl.BlockSpec(memory_space=pl.ANY)] * 2,
        out_specs=[pl.BlockSpec(memory_space=pl.ANY)] * 2,
        scratch_shapes=[V(outT.shape, BF16), V(new.shape, F32), S((2, 1 + new.shape[0]))],
        name="write_out",
    )(outT, new)
    return outT.T, new


def solution(mesh):
    in_specs = (
        P("dp", ("kv", "tp")),
        P(("dp", "kv"), "tp", None, None),
        P(("dp", "kv"), "tp"),
        P(),
        P(None, ("kv", "tp")),
        P(None, ("kv", "tp")),
        P(("kv", "tp"), None),
        P("kv"),
        P("kv", "tp"),
        P("kv", "tp"),
        P("kv", "tp"),
        P("kv", "tp"),
        P("kv", "tp"),
        P("tp"),
        P("tp", "kv"),
        P(),
        P(None, ("kv", "tp")),
        P(None, ("kv", "tp")),
        P(("kv", "tp"), None),
    )
    out_specs = (P("dp", ("kv", "tp")), P(("dp", "kv"), "tp", None, None))
    return jax.shard_map(body, mesh=mesh, in_specs=in_specs, out_specs=out_specs, check_vma=False)
```

```python
import functools

import jax
import jax.numpy as jnp
from jax import lax
from jax.experimental import pallas as pl
from jax.experimental.pallas import tpu as pltpu
from jax.sharding import PartitionSpec as P

EPSILON = 1e-06
GATE_SOFTNESS = 16.0
NY = 4
C = 16
HID = 48
NF = 15
F32 = jnp.float32
BF16 = jnp.bfloat16


def copy_to(src, dst, send, recv, **where):
    return pltpu.make_async_remote_copy(
        src_ref=src,
        dst_ref=dst,
        send_sem=send,
        recv_sem=recv,
        device_id=where,
        device_id_type=pl.DeviceIdType.MESH,
    )


def dot(a, b, ca, cb):
    return lax.dot_general(a, b, (((ca,), (cb,)), ((), ())), preferred_element_type=F32)


def kernel(NZ, FFL, *refs):
    hbm = refs[:19]
    outT, new = refs[19:21]
    local = refs[21:40]
    (
        newv,
        gat1,
        gat2,
        wgu1,
        wgu2,
        wdt1,
        wdt2,
        s0,
        hx,
        wdx,
        ysend,
        yrecv,
        zdirect,
        accf,
        zsend,
        zrecv,
        midg,
        wall,
        wsh,
        wog,
        trn,
        zs,
        zsb,
        zrb,
        ytot,
        mg,
        mgf,
        pj,
        pjr,
        aft,
        ld,
        ag,
        ag_t,
        hx_s,
        wd_s,
        rs_y,
        rs_d,
        rs_z,
        md,
        w_y,
        wo_y,
        pr_z,
        mh,
        fin_s,
    ) = refs[40:]
    (
        sT,
        old,
        dec,
        g1,
        wg1,
        wu1,
        wd1,
        gm,
        wq,
        wk,
        wz,
        wv,
        wo,
        hg,
        wout,
        g2,
        wg2,
        wu2,
        wd2,
    ) = local
    kv = lax.axis_index("kv")
    t = lax.axis_index("tp")
    z = kv // NY
    y = kv % NY
    R = 2 * NY * NZ
    D = NZ * NY * 2 * C

    def zpeer(k):
        return lax.rem(z + k, NZ)

    def ypeer(k):
        return lax.rem(y + k, NY)

    def yfrom(k):
        return lax.rem(y + NY - k, NY)

    def at_z(zz):
        return {"kv": zz * NY + y}

    def at_y(yy):
        return {"kv": z * NY + yy}

    other = {"tp": 1 - t}

    def far_first(i):
        return NZ // 2 + (1 - 2 * lax.rem(i, 2)) * ((i + 1) // 2)

    barrier = pltpu.get_barrier_semaphore()

    def greet(**where):
        pl.semaphore_signal(
            barrier, inc=1, device_id=where, device_id_type=pl.DeviceIdType.MESH
        )

    def greet_z(i, c):
        greet(**at_z(zpeer(far_first(i))))
        return c

    lax.fori_loop(0, NZ - 1, greet_z, 0)
    for k in range(1, NY):
        greet(**at_y(ypeer(k)))
        greet(**at_y(ypeer(k)), **other)
    greet(**other)

    def load(i):
        return pltpu.make_async_copy(hbm[i], local[i], ld.at[i])

    for i in (0, 3, 4, 5, 6, 7, 8, 9, 10, 11, 12, 15, 16, 17, 18, 1, 2, 13, 14):
        load(i).start()

    seq = lax.broadcasted_iota(jnp.int32, (R, R), 0)
    lane = lax.broadcasted_iota(jnp.int32, (R, R), 1)
    home = (lane % NZ) * (2 * NY) + (lane // (2 * NZ)) * 2 + (lane // NZ) % 2
    perm = jnp.where(seq == home, 1.0, 0.0).astype(BF16)
    load(0).wait()
    s0[...] = dot(sT[...], perm, 1, 0).astype(BF16)

    def fold(wgu, wg, wu, gain):
        row = gain[...]
        pad = jnp.zeros((HID - FFL, D), F32)
        for part, w in enumerate((wg, wu)):
            scaled = jnp.concatenate([w[...].astype(F32) * row, pad], axis=0)
            wgu[part * HID : (part + 1) * HID, :] = scaled.astype(BF16)
        if wgu.shape[0] > 2 * HID:
            wgu[2 * HID :, :] = jnp.zeros((wgu.shape[0] - 2 * HID, D), BF16)

    def turn(wdt, wd):
        width = NY * 2 * C
        for b in range(NZ):
            block = wd[:, b * width : (b + 1) * width].astype(F32)
            block = jnp.concatenate([block, jnp.zeros((128 - FFL, width), F32)], axis=0)
            turned = jnp.transpose(block).astype(BF16).reshape(NY, 2, C, 128)
            for p in range(2):
                for yy in range(NY):
                    wdt[p, yy, b] = turned[yy, p]

    for i in (3, 4, 5):
        load(i).wait()
    fold(wgu1, wg1, wu1, g1)
    load(6).wait()
    turn(wdt1, wd1)
    for i in range(7, 13):
        load(i).wait()
    eye = lax.broadcasted_iota(jnp.int32, (2 * C, 2 * C), 0) == lax.broadcasted_iota(
        jnp.int32, (2 * C, 2 * C), 1
    )
    gain_col = jnp.sum(
        jnp.where(eye, jnp.broadcast_to(gm[...], (2 * C, 2 * C)), 0.0), axis=1, keepdims=True
    )
    f = 0
    for w in (wq, wk, wz, wv, wo):
        scaled = (w[...].astype(F32) * gain_col).astype(BF16)
        for j in range(w.shape[1] // 128):
            wall[f] = scaled[:, j * 128 : (j + 1) * 128]
            f += 1
    for f in range(NF - 1, 4 * NY):
        wall[f] = jnp.zeros((2 * C, 128), BF16)
    pl.semaphore_wait(barrier, NZ - 1 + 2 * (NY - 1) + 1)

    sends = []

    def owe(ref, sem):
        sends.append(copy_to(ref, ref, sem, sem, **other).wait_send)

    def got(ref, sem):
        copy_to(ref, ref, sem, sem, **other).wait_recv()

    G = max(NZ // 4, 1)
    NG = NZ // G
    order = [0] + [(i + 1) // 2 if i % 2 else NG - i // 2 for i in range(1, NG)]

    def gather(slot, most, sem, everything=None, pair_sem=None):
        mine = slot(z, 1, y)

        def send(i, c):
            copy_to(mine, mine, sem.at[0], sem.at[1 + z // G], **at_z(zpeer(far_first(i)))).start()
            return c

        lax.fori_loop(0, NZ - 1, send, 0)
        owe(slot(0, NZ - 1, 0), sem.at[0])

        def finish():
            arrival = 2 + NG
            for i in range(NG):
                q = lax.rem(z // G + order[i], NG)
                n = G if i else G - 1
                if n:
                    got(slot(0, n, 0), sem.at[1 + q])
                group = slot(q * G, G, y)
                for j in (2, 1, 3):
                    copy_to(
                        group,
                        group,
                        sem.at[1 + NG],
                        sem.at[arrival + (j - 1) * NG + i],
                        **at_y(ypeer(j)),
                    ).start()
                if pair_sem is not None:
                    copy_to(group, group, pair_sem.at[0], pair_sem.at[1], **other).start()
            for i in range(NG):
                q = lax.rem(z // G + order[i], NG)
                for j in (1, 3, 2):
                    group = slot(q * G, G, yfrom(j))
                    got(group, sem.at[arrival + (j - 1) * NG + i])
                    if pair_sem is not None:
                        copy_to(group, group, pair_sem.at[0], pair_sem.at[1], **other).start()
            owe(most, sem.at[1 + NG])
            if pair_sem is not None:
                got(everything, pair_sem.at[1])
                owe(everything, pair_sem.at[0])

        return finish

    def gated(gate, up):
        return (gate * jax.nn.sigmoid(gate) * up).astype(BF16)

    def half(phase, hidden, wdt, meanwhile, residual):
        hx[phase, 0, 0:HID] = hidden
        hx[phase, 0, HID:] = jnp.zeros((128 - HID, R), BF16)
        hx[phase, 1, HID:] = jnp.zeros((128 - HID, R), BF16)
        units = pl.ds(0, HID)
        copy_to(
            hx.at[phase, 0, units],
            hx.at[phase, 1, units],
            hx_s.at[phase, 0],
            hx_s.at[phase, 1],
            **other,
        ).start()
        owe(hx.at[phase, 0, units], hx_s.at[phase, 0])
        far = [(i, pl.ds(lax.rem(z // G + o, NG) * G, G)) for i, o in enumerate(order[::-1])]
        got(wdx.at[phase], wd_s.at[phase, 1])
        got(hx.at[phase, 1, units], hx_s.at[phase, 1])
        pair_hidden = hx[phase].reshape(256, R)
        for slot, k in ((2, 2), (0, 1), (1, 3), (None, 4)):
            yy = lax.rem(y + k, NY)
            w = [wdt[t, yy].reshape(NZ * C, 128), wdx[phase, yy].reshape(NZ * C, 128)]
            both = dot(jnp.concatenate(w, axis=1), pair_hidden, 1, 0).reshape(NZ, C, R)
            if k == 4:
                break
            ysend[phase, slot] = both.astype(BF16)
            if k == 2:

                def direct(i, c):
                    kz = lax.rem(far_first(i), NZ)
                    zz = zpeer(kz)
                    copy_to(
                        ysend.at[phase, 2, zz],
                        zdirect.at[phase, kz],
                        rs_d.at[phase, 0],
                        rs_d.at[phase, 1],
                        kv=zz * NY + lax.rem(y + 2, NY),
                    ).start()
                    return c

                lax.fori_loop(0, NZ, direct, 0)
                continue
            for i, part in far:
                copy_to(
                    ysend.at[phase, slot, part],
                    yrecv.at[phase, slot, part],
                    rs_y.at[phase, 0],
                    rs_y.at[phase, 1 + i],
                    **at_y(yy),
                ).start()
        accf[phase] = both
        owe(ysend.at[phase, pl.ds(0, 2)], rs_y.at[phase, 0])
        owe(ysend.at[phase, 2], rs_d.at[phase, 0])
        for i, part in far:
            got(yrecv.at[phase, :, part], rs_y.at[phase, 1 + i])
            sums = accf[phase, part]
            for slot in range(2):
                sums = sums + yrecv[phase, slot, part].astype(F32)
            accf[phase, part] = sums
            zsend[phase, part] = sums.astype(BF16)
            for j in range(G):
                if i < NG - 1:
                    zz = part.start + j
                elif j:
                    zz = part.start + lax.rem(z + j, G)
                else:
                    continue
                copy_to(
                    zsend.at[phase, zz],
                    zrecv.at[phase, lax.rem(zz + NZ - z, NZ)],
                    rs_z.at[phase, 0],
                    rs_z.at[phase, 1],
                    **at_z(zz),
                ).start()
        landed = zrecv.at[phase, pl.ds(1, NZ - 1)]
        owe(landed, rs_z.at[phase, 0])
        meanwhile()
        total = accf[phase, z]
        got(landed, rs_z.at[phase, 1])
        got(zdirect.at[phase], rs_d.at[phase, 1])
        for k in range(NZ):
            total = total + zdirect[phase, k].astype(F32)
            if k:
                total = total + zrecv[phase, k].astype(F32)
        return (residual() + 0.5 * total).astype(BF16)

    def share_down(phase, wdt):
        copy_to(
            wdt.at[1 - t], wdx.at[phase], wd_s.at[phase, 0], wd_s.at[phase, 1], **other
        ).start()
        owe(wdx.at[phase], wd_s.at[phase, 0])

    gat1[z, y, t] = s0[...]
    finish = gather(
        lambda zz, n, yy: gat1.at[pl.ds(zz, n), yy, t],
        gat1.at[:, pl.ds(0, NY - 1), t],
        ag.at[0],
        gat1.at[:, :, t],
        ag_t.at[0],
    )
    wsh[y] = wall[pl.ds(4 * y, 4)]
    share_down(0, wdt1)
    finish()
    all_rows = gat1[...].reshape(D, R)
    acc = dot(wgu1[...], all_rows, 1, 0)
    wide = all_rows.astype(F32)
    scale = lax.rsqrt(jnp.sum(wide * wide, axis=0, keepdims=True) / D + EPSILON)

    def share_weights():
        for k in range(1, NY):
            yy = ypeer(k)
            copy_to(wall.at[pl.ds(4 * yy, 4)], wsh.at[y], w_y.at[0], w_y.at[1], **at_y(yy)).start()
        load(14).wait()
        for k in range(1, NY):
            copy_to(wout, wog.at[y], wo_y.at[0], wo_y.at[1], **at_y(ypeer(k))).start()
        owe(wall.at[pl.ds(0, 4 * (NY - 1))], w_y.at[0])
        owe(wog.at[pl.ds(0, NY - 1)], wo_y.at[0])
        wog[y] = wout[...]

    hidden = gated(acc[:HID] * scale, acc[HID:] * scale)
    middle = half(0, hidden, wdt1, share_weights, lambda: s0[...].astype(F32))

    here = midg.at[2 * y + t]
    here[...] = middle
    for k in range(NY):
        where = at_y(ypeer(k))
        copy_to(here, here, md.at[0], md.at[1], **where, **other).start()
        if k:
            copy_to(here, here, md.at[0], md.at[1], **where).start()
    most = midg.at[pl.ds(0, 2 * NY - 1)]
    owe(most, md.at[0])
    got(wsh.at[pl.ds(0, NY - 1)], w_y.at[1])
    got(most, md.at[1])

    turned = jnp.transpose(midg[...].astype(F32).reshape(NY * 2 * C, R))
    trn[...] = turned.reshape(2 * NY, NZ, 128)
    squares = jnp.sum(turned * turned, axis=1, keepdims=True)
    squares = squares * jnp.where(y == NY - 1, 1.0, 0.0)
    lhs = turned.astype(BF16)
    for c in range(4):
        part = dot(lhs, wsh[:, c].reshape(NY * 2 * C, 128), 1, 0)
        if c == 2:
            part = part + squares
        for yy in range(NY):
            for s in range(2):
                at = (yy * 2 + s) * NZ
                zs[pl.ds(yy * 8 + s * 4 + c, NZ, stride=32), :] = part[at : at + NZ]
    zsb[...] = zs[...].astype(BF16).reshape(NZ, NY, 8, 128)

    def send_sums(i, c):
        k = far_first(i)
        zz = zpeer(k)
        for j in (2, 1, 3, 0):
            yy = ypeer(j)
            there = {"kv": zz * NY + yy}
            copy_to(zsb.at[zz, yy], zrb.at[k * NY + y], pr_z.at[0], pr_z.at[1], **there).start()
        return c

    lax.fori_loop(0, NZ - 1, send_sums, 0)
    for j in (2, 1, 3):
        yy = ypeer(j)
        copy_to(zsb.at[z, yy], zrb.at[y], pr_z.at[0], pr_z.at[1], **at_y(yy)).start()
    zrb[y] = zsb[z, y]
    landed = zrb.at[pl.ds(0, NZ * NY - 1)]
    owe(landed, pr_z.at[0])
    for i in (1, 2, 13):
        load(i).wait()
    got(landed, pr_z.at[1])
    for yy in range(NY):
        total = zrb[yy].astype(F32)
        for k in range(1, NZ):
            total = total + zrb[k * NY + yy].astype(F32)
        ytot[yy] = total

    blocks = []
    columns = []
    for s in range(2):
        b = jnp.concatenate([ytot[yy, s * 4 : (s + 1) * 4] for yy in range(NY)], axis=0)
        b = b * lax.rsqrt(b[NF - 1 : NF] / D + EPSILON)
        blocks.append(b)
        logits = b[4:6]
        amounts = jnp.concatenate([dec[s : s + 1, 0:128], dec[s : s + 1, 128:256]], axis=0)
        sig = jnp.minimum(logits, 0.0) - jnp.log(1.0 + jnp.exp(-jnp.abs(logits)))
        decay = jnp.exp(sig / GATE_SOFTNESS - amounts)
        columns += [b[0:2] * 0.125, b[2:4], decay]
    columns.append(jnp.zeros((128 - 12, 128), F32))
    cols = jnp.transpose(jnp.concatenate(columns, axis=0))
    rows = []
    for s in range(2):
        for h in range(4):
            lo = (h % 2) * 64
            q, k_, a = (
                cols[lo : lo + 64, s * 6 + 2 * i + h // 2 : s * 6 + 2 * i + h // 2 + 1]
                for i in range(3)
            )
            b = blocks[s]
            state = a * old[s, h] + k_ * b[6 + h : 7 + h]
            newv[s, h] = state
            read = jnp.sum(q * state, axis=0, keepdims=True)
            normed = read * lax.rsqrt(jnp.mean(read * read, axis=1, keepdims=True) + EPSILON)
            o = b[10 + h : 11 + h]
            rows.append(normed * hg[h : h + 1] * (o * jax.nn.sigmoid(o)))
    mg[z] = jnp.concatenate(rows, axis=0).astype(BF16)

    def send_heads(i, c):
        zz = zpeer(far_first(i))
        copy_to(mg.at[z], mg.at[z], mh.at[0], mh.at[1], **at_z(zz)).start()
        return c

    lax.fori_loop(0, NZ - 1, send_heads, 0)
    owe(mg.at[pl.ds(0, NZ - 1)], mh.at[0])
    out_copy = pltpu.make_async_copy(newv, new, ld.at[0])
    out_copy.start()
    sends.append(out_copy.wait)
    for i in (15, 16, 17, 18):
        load(i).wait()
    fold(wgu2, wg2, wu2, g2)
    turn(wdt2, wd2)
    got(wog.at[pl.ds(0, NY - 1)], wo_y.at[1])
    got(mg.at[pl.ds(0, NZ - 1)], mh.at[1])
    share_down(1, wdt2)
    mgf[...] = mg[...].astype(F32).reshape(NZ * 8, 128)
    heads = []
    for h in range(4):
        pieces = [mgf[pl.ds(s * 4 + h, NZ, stride=8), :] for s in range(2)]
        heads.append(jnp.concatenate(pieces, axis=0))
    mixed = jnp.concatenate(heads, axis=1).astype(BF16)
    product = dot(mixed, wog[...].reshape(NY * 2 * C, 512), 1, 1).astype(BF16)
    pj[...] = product.reshape(2, NZ, NY * 2 * C)
    copy_to(pj.at[1 - t], pjr, fin_s.at[0], fin_s.at[1], **other).start()
    owe(pjr, fin_s.at[0])
    got(pjr, fin_s.at[1])
    attention = pj[t].astype(F32) + pjr[...].astype(F32)

    gat2[z, y, t] = (trn[2 * y + t] + attention).astype(BF16)
    gather(
        lambda zz, n, yy: gat2.at[pl.ds(zz, n), yy, t],
        gat2.at[:, pl.ds(0, NY - 1), t],
        ag.at[1],
        gat2.at[:, :, t],
        ag_t.at[1],
    )()
    all_rows = jnp.concatenate([gat2[i].reshape(R, NY * 2 * C) for i in range(NZ)], axis=1)
    acc = dot(all_rows, wgu2[...], 1, 1)
    wide = all_rows.astype(F32)
    scale = lax.rsqrt(jnp.sum(wide * wide, axis=1, keepdims=True) / D + EPSILON)
    acc = jnp.transpose(acc * scale)

    def own_columns():
        block = gat2[z].astype(F32).reshape(R, NY * 2 * C)
        aft[...] = jnp.transpose(block).reshape(2 * NY, C, R)

    hidden = gated(acc[:HID], acc[HID : 2 * HID])
    result = half(1, hidden, wdt2, own_columns, lambda: aft[2 * y + t])
    outT[...] = dot(result, perm, 1, 1).astype(BF16)
    for wait in sends:
        wait()


def write_out(outT, new, outT_ref, new_ref, o_v, n_v, sem):
    parts = new.shape[0]
    moves = [(outT, o_v, outT_ref)] + [(new.at[i], n_v.at[i], new_ref.at[i]) for i in range(parts)]
    ins = [pltpu.make_async_copy(a, v, sem.at[0, i]) for i, (a, v, _) in enumerate(moves)]
    outs = [pltpu.make_async_copy(v, b, sem.at[1, i]) for i, (_, v, b) in enumerate(moves)]
    for c in ins:
        c.start()
    for a, b in zip(ins, outs):
        a.wait()
        b.start()
    for c in outs:
        c.wait()


def body(
    stream,
    old_state,
    decay_amounts,
    first_gain,
    first_gate,
    first_up,
    first_down,
    mixer_gain,
    query_weight,
    key_weight,
    decay_weight,
    value_weight,
    output_gate_weight,
    head_gain,
    output_weight,
    second_gain,
    second_gate,
    second_up,
    second_down,
):
    NZ = lax.axis_size("kv") // NY
    R = 2 * NY * NZ
    D = NY * NZ * 2 * C
    NG = NZ // max(NZ // 4, 1)
    V = pltpu.VMEM
    S = pltpu.SemaphoreType.DMA
    arrays = (
        stream.T,
        old_state,
        decay_amounts,
        first_gain.reshape(1, D),
        first_gate.T,
        first_up.T,
        first_down,
        mixer_gain.reshape(1, 2 * C),
        query_weight,
        key_weight,
        decay_weight,
        value_weight,
        output_gate_weight,
        head_gain.reshape(4, 128),
        output_weight.T,
        second_gain.reshape(1, D),
        second_gate.T,
        second_up.T,
        second_down,
    )
    outT, new = pl.pallas_call(
        functools.partial(kernel, NZ, first_gate.shape[1]),
        out_shape=(
            jax.ShapeDtypeStruct((C, R), BF16),
            jax.ShapeDtypeStruct(old_state.shape, F32),
        ),
        in_specs=[pl.BlockSpec(memory_space=pl.ANY)] * 19,
        out_specs=[pl.BlockSpec(memory_space=pltpu.VMEM), pl.BlockSpec(memory_space=pl.ANY)],
        scratch_shapes=[V(a.shape, a.dtype) for a in arrays]
        + [
            V(old_state.shape, F32),
            V((NZ, NY, 2, C, R), BF16),
            V((NZ, NY, 2, NZ, NY * 2 * C), BF16),
            V((2 * HID, D), BF16),
            V((128, D), BF16),
            V((2, NY, NZ, C, 128), BF16),
            V((2, NY, NZ, C, 128), BF16),
            V((C, R), BF16),
            V((2, 2, 128, R), BF16),
            V((2, NY, NZ, C, 128), BF16),
            V((2, 3, NZ, C, R), BF16),
            V((2, 2, NZ, C, R), BF16),
            V((2, NZ, C, R), BF16),
            V((2, NZ, C, R), F32),
            V((2, NZ, C, R), BF16),
            V((2, NZ, C, R), BF16),
            V((2 * NY, C, R), BF16),
            V((4 * NY, 2 * C, 128), BF16),
            V((NY, 4, 2 * C, 128), BF16),
            V((NY, 2 * C, 512), BF16),
            V((2 * NY, NZ, 128), F32),
            V((NZ * 32, 128), F32),
            V((NZ, NY, 8, 128), BF16),
            V((NZ * NY, 8, 128), BF16),
            V((NY, 8, 128), F32),
            V((NZ, 8, 128), BF16),
            V((NZ * 8, 128), F32),
            V((2, NZ, NY * 2 * C), BF16),
            V((NZ, NY * 2 * C), BF16),
            V((2 * NY, C, R), F32),
            S((19,)),
            S((2, 2 + NY * NG)),
            S((2, 2)),
            S((2, 2)),
            S((2, 2)),
            S((2, 1 + NG)),
            S((2, 2)),
            S((2, 2)),
            S((2,)),
            S((2,)),
            S((2,)),
            S((2,)),
            S((2,)),
            S((2,)),
        ],
        compiler_params=pltpu.CompilerParams(collective_id=0, has_side_effects=True),
        name="layer",
    )(*arrays)
    outT, new = pl.pallas_call(
        write_out,
        out_shape=(
            jax.ShapeDtypeStruct(outT.shape, BF16),
            jax.ShapeDtypeStruct(new.shape, F32),
        ),
        in_specs=[pl.BlockSpec(memory_space=pl.ANY)] * 2,
        out_specs=[pl.BlockSpec(memory_space=pl.ANY)] * 2,
        scratch_shapes=[V(outT.shape, BF16), V(new.shape, F32), S((2, 1 + new.shape[0]))],
        name="write_out",
    )(outT, new)
    return outT.T, new


def solution(mesh):
    in_specs = (
        P("dp", ("kv", "tp")),
        P(("dp", "kv"), "tp", None, None),
        P(("dp", "kv"), "tp"),
        P(),
        P(None, ("kv", "tp")),
        P(None, ("kv", "tp")),
        P(("kv", "tp"), None),
        P("kv"),
        P("kv", "tp"),
        P("kv", "tp"),
        P("kv", "tp"),
        P("kv", "tp"),
        P("kv", "tp"),
        P("tp"),
        P("tp", "kv"),
        P(),
        P(None, ("kv", "tp")),
        P(None, ("kv", "tp")),
        P(("kv", "tp"), None),
    )
    out_specs = (P("dp", ("kv", "tp")), P(("dp", "kv"), "tp", None, None))
    return jax.shard_map(body, mesh=mesh, in_specs=in_specs, out_specs=out_specs, check_vma=False)
```

```python
import functools

import jax
import jax.numpy as jnp
from jax import lax
from jax.experimental import pallas as pl
from jax.experimental.pallas import tpu as pltpu
from jax.sharding import PartitionSpec as P

EPSILON = 1e-06
GATE_SOFTNESS = 16.0
NY = 4
C = 16
HID = 48
NF = 15
F32 = jnp.float32
BF16 = jnp.bfloat16


def copy_to(src, dst, send, recv, **where):
    return pltpu.make_async_remote_copy(
        src_ref=src,
        dst_ref=dst,
        send_sem=send,
        recv_sem=recv,
        device_id=where,
        device_id_type=pl.DeviceIdType.MESH,
    )


def dot(a, b, ca, cb):
    return lax.dot_general(a, b, (((ca,), (cb,)), ((), ())), preferred_element_type=F32)


def kernel(NZ, FFL, *refs):
    hbm = refs[:19]
    outT, new = refs[19:21]
    local = refs[21:40]
    (
        newv,
        gat1,
        gat2,
        wgu1,
        wgu2,
        wdt1,
        wdt2,
        s0,
        hx,
        wdx,
        ysend,
        yrecv,
        zdirect,
        accf,
        zsend,
        zrecv,
        midg,
        wall,
        wsh,
        wog,
        trn,
        zs,
        zsb,
        zrb,
        ytot,
        mg,
        mgf,
        pj,
        pjr,
        aft,
        ld,
        ag,
        ag_t,
        hx_s,
        wd_s,
        rs_y,
        rs_d,
        rs_z,
        md,
        w_y,
        wo_y,
        pr_z,
        mh,
        fin_s,
    ) = refs[40:]
    (
        sT,
        old,
        dec,
        g1,
        wg1,
        wu1,
        wd1,
        gm,
        wq,
        wk,
        wz,
        wv,
        wo,
        hg,
        wout,
        g2,
        wg2,
        wu2,
        wd2,
    ) = local
    kv = lax.axis_index("kv")
    t = lax.axis_index("tp")
    z = kv // NY
    y = kv % NY
    R = 2 * NY * NZ
    D = NZ * NY * 2 * C

    def zpeer(k):
        return lax.rem(z + k, NZ)

    def ypeer(k):
        return lax.rem(y + k, NY)

    def yfrom(k):
        return lax.rem(y + NY - k, NY)

    def at_z(zz):
        return {"kv": zz * NY + y}

    def at_y(yy):
        return {"kv": z * NY + yy}

    other = {"tp": 1 - t}

    def far_first(i):
        return NZ // 2 + (1 - 2 * lax.rem(i, 2)) * ((i + 1) // 2)

    barrier = pltpu.get_barrier_semaphore()

    def greet(**where):
        pl.semaphore_signal(
            barrier, inc=1, device_id=where, device_id_type=pl.DeviceIdType.MESH
        )

    def greet_z(i, c):
        greet(**at_z(zpeer(far_first(i))))
        return c

    lax.fori_loop(0, NZ - 1, greet_z, 0)
    for k in range(1, NY):
        greet(**at_y(ypeer(k)))
        greet(**at_y(ypeer(k)), **other)
    greet(**other)

    def load(i):
        return pltpu.make_async_copy(hbm[i], local[i], ld.at[i])

    for i in (0, 3, 4, 5, 6, 7, 8, 9, 10, 11, 12, 15, 16, 17, 18, 1, 2, 13, 14):
        load(i).start()

    seq = lax.broadcasted_iota(jnp.int32, (R, R), 0)
    lane = lax.broadcasted_iota(jnp.int32, (R, R), 1)
    home = (lane % NZ) * (2 * NY) + (lane // (2 * NZ)) * 2 + (lane // NZ) % 2
    perm = jnp.where(seq == home, 1.0, 0.0).astype(BF16)
    load(0).wait()
    s0[...] = dot(sT[...], perm, 1, 0).astype(BF16)

    def fold(wgu, wg, wu, gain):
        row = gain[...]
        pad = jnp.zeros((HID - FFL, D), F32)
        for part, w in enumerate((wg, wu)):
            scaled = jnp.concatenate([w[...].astype(F32) * row, pad], axis=0)
            wgu[part * HID : (part + 1) * HID, :] = scaled.astype(BF16)
        if wgu.shape[0] > 2 * HID:
            wgu[2 * HID :, :] = jnp.zeros((wgu.shape[0] - 2 * HID, D), BF16)

    def turn(wdt, wd):
        width = NY * 2 * C
        for b in range(NZ):
            block = wd[:, b * width : (b + 1) * width].astype(F32)
            block = jnp.concatenate([block, jnp.zeros((128 - FFL, width), F32)], axis=0)
            turned = jnp.transpose(block).astype(BF16).reshape(NY, 2, C, 128)
            for p in range(2):
                for yy in range(NY):
                    wdt[p, yy, b] = turned[yy, p]

    for i in (3, 4, 5):
        load(i).wait()
    fold(wgu1, wg1, wu1, g1)
    load(6).wait()
    turn(wdt1, wd1)
    for i in range(7, 13):
        load(i).wait()
    eye = lax.broadcasted_iota(jnp.int32, (2 * C, 2 * C), 0) == lax.broadcasted_iota(
        jnp.int32, (2 * C, 2 * C), 1
    )
    gain_col = jnp.sum(
        jnp.where(eye, jnp.broadcast_to(gm[...], (2 * C, 2 * C)), 0.0), axis=1, keepdims=True
    )
    f = 0
    for w in (wq, wk, wz, wv, wo):
        scaled = (w[...].astype(F32) * gain_col).astype(BF16)
        for j in range(w.shape[1] // 128):
            wall[f] = scaled[:, j * 128 : (j + 1) * 128]
            f += 1
    for f in range(NF - 1, 4 * NY):
        wall[f] = jnp.zeros((2 * C, 128), BF16)
    pl.semaphore_wait(barrier, NZ - 1 + 2 * (NY - 1) + 1)

    sends = []

    def owe(ref, sem):
        sends.append(copy_to(ref, ref, sem, sem, **other).wait_send)

    def got(ref, sem):
        copy_to(ref, ref, sem, sem, **other).wait_recv()

    G = max(NZ // 8, 1)
    NG = NZ // G
    order = [0] + [(i + 1) // 2 if i % 2 else NG - i // 2 for i in range(1, NG)]

    def gather(slot, columns, sem, pair_sem):
        mine = slot(z, 1, y)

        def send(i, c):
            copy_to(mine, mine, sem.at[0], sem.at[1 + z // G], **at_z(zpeer(far_first(i)))).start()
            return c

        lax.fori_loop(0, NZ - 1, send, 0)
        owe(slot(0, NZ - 1, 0), sem.at[0])

        def finish():
            arrival = 2 + NG
            for i in range(NG):
                q = lax.rem(z // G + order[i], NG)
                n = G if i else G - 1
                if n:
                    got(slot(0, n, 0), sem.at[1 + q])
                group = slot(q * G, G, y)
                for j in (2, 1, 3):
                    copy_to(
                        group,
                        group,
                        sem.at[1 + NG],
                        sem.at[arrival + i],
                        **at_y(ypeer(j)),
                    ).start()
                copy_to(group, group, pair_sem.at[0], pair_sem.at[1], **other).start()
            for i in range(NG):
                q = lax.rem(z // G + order[i], NG)
                got(columns(0, G, NY - 1), sem.at[arrival + i])
                for j in (1, 3, 2):
                    group = slot(q * G, G, yfrom(j))
                    copy_to(group, group, pair_sem.at[0], pair_sem.at[1], **other).start()
            owe(columns(0, NZ, NY - 1), sem.at[1 + NG])
            everything = columns(0, NZ, NY)
            got(everything, pair_sem.at[1])
            owe(everything, pair_sem.at[0])

        return finish

    def gated(gate, up):
        return (gate * jax.nn.sigmoid(gate) * up).astype(BF16)

    def half(phase, hidden, wdt, meanwhile, residual):
        hx[phase, 0, 0:HID] = hidden
        hx[phase, 0, HID:] = jnp.zeros((128 - HID, R), BF16)
        hx[phase, 1, HID:] = jnp.zeros((128 - HID, R), BF16)
        units = pl.ds(0, HID)
        copy_to(
            hx.at[phase, 0, units],
            hx.at[phase, 1, units],
            hx_s.at[phase, 0],
            hx_s.at[phase, 1],
            **other,
        ).start()
        owe(hx.at[phase, 0, units], hx_s.at[phase, 0])
        far = [(i, pl.ds(lax.rem(z // G + o, NG) * G, G)) for i, o in enumerate(order[::-1])]
        got(wdx.at[phase], wd_s.at[phase, 1])
        got(hx.at[phase, 1, units], hx_s.at[phase, 1])
        pair_hidden = hx[phase].reshape(256, R)
        for slot, k in ((2, 2), (0, 1), (1, 3), (None, 4)):
            yy = lax.rem(y + k, NY)
            w = [wdt[t, yy].reshape(NZ * C, 128), wdx[phase, yy].reshape(NZ * C, 128)]
            both = dot(jnp.concatenate(w, axis=1), pair_hidden, 1, 0).reshape(NZ, C, R)
            if k == 4:
                break
            ysend[phase, slot] = both.astype(BF16)
            if k == 2:

                def direct(i, c):
                    kz = lax.rem(far_first(i), NZ)
                    zz = zpeer(kz)
                    copy_to(
                        ysend.at[phase, 2, zz],
                        zdirect.at[phase, kz],
                        rs_d.at[phase, 0],
                        rs_d.at[phase, 1],
                        kv=zz * NY + lax.rem(y + 2, NY),
                    ).start()
                    return c

                lax.fori_loop(0, NZ, direct, 0)
                continue
            for i, part in far:
                copy_to(
                    ysend.at[phase, slot, part],
                    yrecv.at[phase, slot, part],
                    rs_y.at[phase, 0],
                    rs_y.at[phase, 1 + i],
                    **at_y(yy),
                ).start()
        accf[phase] = both
        owe(ysend.at[phase, pl.ds(0, 2)], rs_y.at[phase, 0])
        owe(ysend.at[phase, 2], rs_d.at[phase, 0])
        for i, part in far:
            got(yrecv.at[phase, :, part], rs_y.at[phase, 1 + i])
            sums = accf[phase, part]
            for slot in range(2):
                sums = sums + yrecv[phase, slot, part].astype(F32)
            accf[phase, part] = sums
            zsend[phase, part] = sums.astype(BF16)
            for j in range(G):
                if i < NG - 1:
                    zz = part.start + j
                elif j:
                    zz = part.start + lax.rem(z + j, G)
                else:
                    continue
                copy_to(
                    zsend.at[phase, zz],
                    zrecv.at[phase, lax.rem(zz + NZ - z, NZ)],
                    rs_z.at[phase, 0],
                    rs_z.at[phase, 1],
                    **at_z(zz),
                ).start()
        landed = zrecv.at[phase, pl.ds(1, NZ - 1)]
        owe(landed, rs_z.at[phase, 0])
        meanwhile()
        total = accf[phase, z]
        got(landed, rs_z.at[phase, 1])
        got(zdirect.at[phase], rs_d.at[phase, 1])
        for k in range(NZ):
            total = total + zdirect[phase, k].astype(F32)
            if k:
                total = total + zrecv[phase, k].astype(F32)
        return (residual() + 0.5 * total).astype(BF16)

    def share_down(phase, wdt):
        copy_to(
            wdt.at[1 - t], wdx.at[phase], wd_s.at[phase, 0], wd_s.at[phase, 1], **other
        ).start()
        owe(wdx.at[phase], wd_s.at[phase, 0])

    gat1[z, y, t] = s0[...]
    finish = gather(
        lambda zz, n, yy: gat1.at[pl.ds(zz, n), yy, t],
        lambda zz, n, m: gat1.at[pl.ds(zz, n), pl.ds(0, m), t],
        ag.at[0],
        ag_t.at[0],
    )
    wsh[y] = wall[pl.ds(4 * y, 4)]
    share_down(0, wdt1)
    finish()
    all_rows = gat1[...].reshape(D, R)
    acc = dot(wgu1[...], all_rows, 1, 0)
    wide = all_rows.astype(F32)
    scale = lax.rsqrt(jnp.sum(wide * wide, axis=0, keepdims=True) / D + EPSILON)

    def share_weights():
        for k in range(1, NY):
            yy = ypeer(k)
            copy_to(wall.at[pl.ds(4 * yy, 4)], wsh.at[y], w_y.at[0], w_y.at[1], **at_y(yy)).start()
        load(14).wait()
        for k in range(1, NY):
            copy_to(wout, wog.at[y], wo_y.at[0], wo_y.at[1], **at_y(ypeer(k))).start()
        owe(wall.at[pl.ds(0, 4 * (NY - 1))], w_y.at[0])
        owe(wog.at[pl.ds(0, NY - 1)], wo_y.at[0])
        wog[y] = wout[...]

    hidden = gated(acc[:HID] * scale, acc[HID:] * scale)
    middle = half(0, hidden, wdt1, share_weights, lambda: s0[...].astype(F32))

    here = midg.at[2 * y + t]
    here[...] = middle
    for k in range(NY):
        where = at_y(ypeer(k))
        copy_to(here, here, md.at[0], md.at[1], **where, **other).start()
        if k:
            copy_to(here, here, md.at[0], md.at[1], **where).start()
    most = midg.at[pl.ds(0, 2 * NY - 1)]
    owe(most, md.at[0])
    got(wsh.at[pl.ds(0, NY - 1)], w_y.at[1])
    got(most, md.at[1])

    turned = jnp.transpose(midg[...].astype(F32).reshape(NY * 2 * C, R))
    trn[...] = turned.reshape(2 * NY, NZ, 128)
    squares = jnp.sum(turned * turned, axis=1, keepdims=True)
    squares = squares * jnp.where(y == NY - 1, 1.0, 0.0)
    lhs = turned.astype(BF16)
    for c in range(4):
        part = dot(lhs, wsh[:, c].reshape(NY * 2 * C, 128), 1, 0)
        if c == 2:
            part = part + squares
        for yy in range(NY):
            for s in range(2):
                at = (yy * 2 + s) * NZ
                zs[pl.ds(yy * 8 + s * 4 + c, NZ, stride=32), :] = part[at : at + NZ]
    zsb[...] = zs[...].astype(BF16).reshape(NZ, NY, 8, 128)

    def send_sums(i, c):
        k = far_first(i)
        zz = zpeer(k)
        for j in (2, 1, 3, 0):
            yy = ypeer(j)
            there = {"kv": zz * NY + yy}
            copy_to(zsb.at[zz, yy], zrb.at[k * NY + y], pr_z.at[0], pr_z.at[1], **there).start()
        return c

    lax.fori_loop(0, NZ - 1, send_sums, 0)
    for j in (2, 1, 3):
        yy = ypeer(j)
        copy_to(zsb.at[z, yy], zrb.at[y], pr_z.at[0], pr_z.at[1], **at_y(yy)).start()
    zrb[y] = zsb[z, y]
    landed = zrb.at[pl.ds(0, NZ * NY - 1)]
    owe(landed, pr_z.at[0])
    for i in (1, 2, 13):
        load(i).wait()
    got(landed, pr_z.at[1])
    for yy in range(NY):
        total = zrb[yy].astype(F32)
        for k in range(1, NZ):
            total = total + zrb[k * NY + yy].astype(F32)
        ytot[yy] = total

    blocks = []
    columns = []
    for s in range(2):
        b = jnp.concatenate([ytot[yy, s * 4 : (s + 1) * 4] for yy in range(NY)], axis=0)
        b = b * lax.rsqrt(b[NF - 1 : NF] / D + EPSILON)
        blocks.append(b)
        logits = b[4:6]
        amounts = jnp.concatenate([dec[s : s + 1, 0:128], dec[s : s + 1, 128:256]], axis=0)
        sig = jnp.minimum(logits, 0.0) - jnp.log(1.0 + jnp.exp(-jnp.abs(logits)))
        decay = jnp.exp(sig / GATE_SOFTNESS - amounts)
        columns += [b[0:2] * 0.125, b[2:4], decay]
    columns.append(jnp.zeros((128 - 12, 128), F32))
    cols = jnp.transpose(jnp.concatenate(columns, axis=0))
    rows = []
    for s in range(2):
        for h in range(4):
            lo = (h % 2) * 64
            q, k_, a = (
                cols[lo : lo + 64, s * 6 + 2 * i + h // 2 : s * 6 + 2 * i + h // 2 + 1]
                for i in range(3)
            )
            b = blocks[s]
            state = a * old[s, h] + k_ * b[6 + h : 7 + h]
            newv[s, h] = state
            read = jnp.sum(q * state, axis=0, keepdims=True)
            normed = read * lax.rsqrt(jnp.mean(read * read, axis=1, keepdims=True) + EPSILON)
            o = b[10 + h : 11 + h]
            rows.append(normed * hg[h : h + 1] * (o * jax.nn.sigmoid(o)))
    mg[z] = jnp.concatenate(rows, axis=0).astype(BF16)

    def send_heads(i, c):
        zz = zpeer(far_first(i))
        copy_to(mg.at[z], mg.at[z], mh.at[0], mh.at[1], **at_z(zz)).start()
        return c

    lax.fori_loop(0, NZ - 1, send_heads, 0)
    owe(mg.at[pl.ds(0, NZ - 1)], mh.at[0])
    out_copy = pltpu.make_async_copy(newv, new, ld.at[0])
    out_copy.start()
    sends.append(out_copy.wait)
    for i in (15, 16, 17, 18):
        load(i).wait()
    fold(wgu2, wg2, wu2, g2)
    turn(wdt2, wd2)
    got(wog.at[pl.ds(0, NY - 1)], wo_y.at[1])
    got(mg.at[pl.ds(0, NZ - 1)], mh.at[1])
    share_down(1, wdt2)
    mgf[...] = mg[...].astype(F32).reshape(NZ * 8, 128)
    heads = []
    for h in range(4):
        pieces = [mgf[pl.ds(s * 4 + h, NZ, stride=8), :] for s in range(2)]
        heads.append(jnp.concatenate(pieces, axis=0))
    mixed = jnp.concatenate(heads, axis=1).astype(BF16)
    product = dot(mixed, wog[...].reshape(NY * 2 * C, 512), 1, 1).astype(BF16)
    pj[...] = product.reshape(2, NZ, NY * 2 * C)
    copy_to(pj.at[1 - t], pjr, fin_s.at[0], fin_s.at[1], **other).start()
    owe(pjr, fin_s.at[0])
    got(pjr, fin_s.at[1])
    attention = pj[t].astype(F32) + pjr[...].astype(F32)

    gat2[z, y, t] = (trn[2 * y + t] + attention).astype(BF16)
    gather(
        lambda zz, n, yy: gat2.at[pl.ds(zz, n), yy, t],
        lambda zz, n, m: gat2.at[pl.ds(zz, n), pl.ds(0, m), t],
        ag.at[1],
        ag_t.at[1],
    )()
    all_rows = jnp.concatenate([gat2[i].reshape(R, NY * 2 * C) for i in range(NZ)], axis=1)
    acc = dot(all_rows, wgu2[...], 1, 1)
    wide = all_rows.astype(F32)
    scale = lax.rsqrt(jnp.sum(wide * wide, axis=1, keepdims=True) / D + EPSILON)
    acc = jnp.transpose(acc * scale)

    def own_columns():
        block = gat2[z].astype(F32).reshape(R, NY * 2 * C)
        aft[...] = jnp.transpose(block).reshape(2 * NY, C, R)

    hidden = gated(acc[:HID], acc[HID : 2 * HID])
    result = half(1, hidden, wdt2, own_columns, lambda: aft[2 * y + t])
    outT[...] = dot(result, perm, 1, 1).astype(BF16)
    for wait in sends:
        wait()


def write_out(outT, new, outT_ref, new_ref, o_v, n_v, sem):
    parts = new.shape[0]
    moves = [(outT, o_v, outT_ref)] + [(new.at[i], n_v.at[i], new_ref.at[i]) for i in range(parts)]
    ins = [pltpu.make_async_copy(a, v, sem.at[0, i]) for i, (a, v, _) in enumerate(moves)]
    outs = [pltpu.make_async_copy(v, b, sem.at[1, i]) for i, (_, v, b) in enumerate(moves)]
    for c in ins:
        c.start()
    for a, b in zip(ins, outs):
        a.wait()
        b.start()
    for c in outs:
        c.wait()


def body(
    stream,
    old_state,
    decay_amounts,
    first_gain,
    first_gate,
    first_up,
    first_down,
    mixer_gain,
    query_weight,
    key_weight,
    decay_weight,
    value_weight,
    output_gate_weight,
    head_gain,
    output_weight,
    second_gain,
    second_gate,
    second_up,
    second_down,
):
    NZ = lax.axis_size("kv") // NY
    R = 2 * NY * NZ
    D = NY * NZ * 2 * C
    NG = NZ // max(NZ // 8, 1)
    V = pltpu.VMEM
    S = pltpu.SemaphoreType.DMA
    arrays = (
        stream.T,
        old_state,
        decay_amounts,
        first_gain.reshape(1, D),
        first_gate.T,
        first_up.T,
        first_down,
        mixer_gain.reshape(1, 2 * C),
        query_weight,
        key_weight,
        decay_weight,
        value_weight,
        output_gate_weight,
        head_gain.reshape(4, 128),
        output_weight.T,
        second_gain.reshape(1, D),
        second_gate.T,
        second_up.T,
        second_down,
    )
    outT, new = pl.pallas_call(
        functools.partial(kernel, NZ, first_gate.shape[1]),
        out_shape=(
            jax.ShapeDtypeStruct((C, R), BF16),
            jax.ShapeDtypeStruct(old_state.shape, F32),
        ),
        in_specs=[pl.BlockSpec(memory_space=pl.ANY)] * 19,
        out_specs=[pl.BlockSpec(memory_space=pltpu.VMEM), pl.BlockSpec(memory_space=pl.ANY)],
        scratch_shapes=[V(a.shape, a.dtype) for a in arrays]
        + [
            V(old_state.shape, F32),
            V((NZ, NY, 2, C, R), BF16),
            V((NZ, NY, 2, NZ, NY * 2 * C), BF16),
            V((2 * HID, D), BF16),
            V((128, D), BF16),
            V((2, NY, NZ, C, 128), BF16),
            V((2, NY, NZ, C, 128), BF16),
            V((C, R), BF16),
            V((2, 2, 128, R), BF16),
            V((2, NY, NZ, C, 128), BF16),
            V((2, 3, NZ, C, R), BF16),
            V((2, 2, NZ, C, R), BF16),
            V((2, NZ, C, R), BF16),
            V((2, NZ, C, R), F32),
            V((2, NZ, C, R), BF16),
            V((2, NZ, C, R), BF16),
            V((2 * NY, C, R), BF16),
            V((4 * NY, 2 * C, 128), BF16),
            V((NY, 4, 2 * C, 128), BF16),
            V((NY, 2 * C, 512), BF16),
            V((2 * NY, NZ, 128), F32),
            V((NZ * 32, 128), F32),
            V((NZ, NY, 8, 128), BF16),
            V((NZ * NY, 8, 128), BF16),
            V((NY, 8, 128), F32),
            V((NZ, 8, 128), BF16),
            V((NZ * 8, 128), F32),
            V((2, NZ, NY * 2 * C), BF16),
            V((NZ, NY * 2 * C), BF16),
            V((2 * NY, C, R), F32),
            S((19,)),
            S((2, 2 + 2 * NG)),
            S((2, 2)),
            S((2, 2)),
            S((2, 2)),
            S((2, 1 + NG)),
            S((2, 2)),
            S((2, 2)),
            S((2,)),
            S((2,)),
            S((2,)),
            S((2,)),
            S((2,)),
            S((2,)),
        ],
        compiler_params=pltpu.CompilerParams(collective_id=0, has_side_effects=True),
        name="layer",
    )(*arrays)
    outT, new = pl.pallas_call(
        write_out,
        out_shape=(
            jax.ShapeDtypeStruct(outT.shape, BF16),
            jax.ShapeDtypeStruct(new.shape, F32),
        ),
        in_specs=[pl.BlockSpec(memory_space=pl.ANY)] * 2,
        out_specs=[pl.BlockSpec(memory_space=pl.ANY)] * 2,
        scratch_shapes=[V(outT.shape, BF16), V(new.shape, F32), S((2, 1 + new.shape[0]))],
        name="write_out",
    )(outT, new)
    return outT.T, new


def solution(mesh):
    in_specs = (
        P("dp", ("kv", "tp")),
        P(("dp", "kv"), "tp", None, None),
        P(("dp", "kv"), "tp"),
        P(),
        P(None, ("kv", "tp")),
        P(None, ("kv", "tp")),
        P(("kv", "tp"), None),
        P("kv"),
        P("kv", "tp"),
        P("kv", "tp"),
        P("kv", "tp"),
        P("kv", "tp"),
        P("kv", "tp"),
        P("tp"),
        P("tp", "kv"),
        P(),
        P(None, ("kv", "tp")),
        P(None, ("kv", "tp")),
        P(("kv", "tp"), None),
    )
    out_specs = (P("dp", ("kv", "tp")), P(("dp", "kv"), "tp", None, None))
    return jax.shard_map(body, mesh=mesh, in_specs=in_specs, out_specs=out_specs, check_vma=False)
```

```python
import functools

import jax
import jax.numpy as jnp
from jax import lax
from jax.experimental import pallas as pl
from jax.experimental.pallas import tpu as pltpu
from jax.sharding import PartitionSpec as P

EPSILON = 1e-06
GATE_SOFTNESS = 16.0
NY = 4
C = 16
HID = 48
NF = 15
F32 = jnp.float32
BF16 = jnp.bfloat16


def copy_to(src, dst, send, recv, **where):
    return pltpu.make_async_remote_copy(
        src_ref=src,
        dst_ref=dst,
        send_sem=send,
        recv_sem=recv,
        device_id=where,
        device_id_type=pl.DeviceIdType.MESH,
    )


def dot(a, b, ca, cb):
    return lax.dot_general(a, b, (((ca,), (cb,)), ((), ())), preferred_element_type=F32)


def kernel(NZ, FFL, *refs):
    hbm = refs[:19]
    outT, new = refs[19:21]
    local = refs[21:40]
    (
        newv,
        gat1,
        gat2,
        wgu1,
        wgu2,
        wdt1,
        wdt2,
        s0,
        hx,
        wdx,
        ysend,
        yrecv,
        zdirect,
        accf,
        zsend,
        zrecv,
        midg,
        wall,
        wsh,
        wog,
        trn,
        zs,
        zsb,
        zrb,
        ytot,
        mg,
        mgf,
        pj,
        pjr,
        aft,
        ld,
        ag,
        ag_t,
        hx_s,
        wd_s,
        rs_y,
        rs_d,
        rs_z,
        md,
        w_y,
        wo_y,
        pr_z,
        mh,
        fin_s,
    ) = refs[40:]
    (
        sT,
        old,
        dec,
        g1,
        wg1,
        wu1,
        wd1,
        gm,
        wq,
        wk,
        wz,
        wv,
        wo,
        hg,
        wout,
        g2,
        wg2,
        wu2,
        wd2,
    ) = local
    kv = lax.axis_index("kv")
    t = lax.axis_index("tp")
    z = kv // NY
    y = kv % NY
    R = 2 * NY * NZ
    D = NZ * NY * 2 * C

    def zpeer(k):
        return lax.rem(z + k, NZ)

    def ypeer(k):
        return lax.rem(y + k, NY)

    def yfrom(k):
        return lax.rem(y + NY - k, NY)

    def at_z(zz):
        return {"kv": zz * NY + y}

    def at_y(yy):
        return {"kv": z * NY + yy}

    other = {"tp": 1 - t}

    def far_first(i):
        return NZ // 2 + (1 - 2 * lax.rem(i, 2)) * ((i + 1) // 2)

    barrier = pltpu.get_barrier_semaphore()

    def greet(**where):
        pl.semaphore_signal(
            barrier, inc=1, device_id=where, device_id_type=pl.DeviceIdType.MESH
        )

    def greet_z(i, c):
        greet(**at_z(zpeer(far_first(i))))
        return c

    lax.fori_loop(0, NZ - 1, greet_z, 0)
    for k in range(1, NY):
        greet(**at_y(ypeer(k)))
        greet(**at_y(ypeer(k)), **other)
    greet(**other)

    def load(i):
        return pltpu.make_async_copy(hbm[i], local[i], ld.at[i])

    for i in (0, 3, 4, 5, 6, 7, 8, 9, 10, 11, 12, 15, 16, 17, 18, 1, 2, 13, 14):
        load(i).start()

    seq = lax.broadcasted_iota(jnp.int32, (R, R), 0)
    lane = lax.broadcasted_iota(jnp.int32, (R, R), 1)
    home = (lane % NZ) * (2 * NY) + (lane // (2 * NZ)) * 2 + (lane // NZ) % 2
    perm = jnp.where(seq == home, 1.0, 0.0).astype(BF16)
    load(0).wait()
    s0[...] = dot(sT[...], perm, 1, 0).astype(BF16)

    def fold(wgu, wg, wu, gain):
        row = gain[...]
        pad = jnp.zeros((HID - FFL, D), F32)
        for part, w in enumerate((wg, wu)):
            scaled = jnp.concatenate([w[...].astype(F32) * row, pad], axis=0)
            wgu[part * HID : (part + 1) * HID, :] = scaled.astype(BF16)
        if wgu.shape[0] > 2 * HID:
            wgu[2 * HID :, :] = jnp.zeros((wgu.shape[0] - 2 * HID, D), BF16)

    def turn(wdt, wd):
        width = NY * 2 * C
        for b in range(NZ):
            block = wd[:, b * width : (b + 1) * width].astype(F32)
            block = jnp.concatenate([block, jnp.zeros((128 - FFL, width), F32)], axis=0)
            turned = jnp.transpose(block).astype(BF16).reshape(NY, 2, C, 128)
            for p in range(2):
                for yy in range(NY):
                    wdt[p, yy, b] = turned[yy, p]

    for i in (3, 4, 5):
        load(i).wait()
    fold(wgu1, wg1, wu1, g1)
    load(6).wait()
    turn(wdt1, wd1)
    for i in range(7, 13):
        load(i).wait()
    eye = lax.broadcasted_iota(jnp.int32, (2 * C, 2 * C), 0) == lax.broadcasted_iota(
        jnp.int32, (2 * C, 2 * C), 1
    )
    gain_col = jnp.sum(
        jnp.where(eye, jnp.broadcast_to(gm[...], (2 * C, 2 * C)), 0.0), axis=1, keepdims=True
    )
    f = 0
    for w in (wq, wk, wz, wv, wo):
        scaled = (w[...].astype(F32) * gain_col).astype(BF16)
        for j in range(w.shape[1] // 128):
            wall[f] = scaled[:, j * 128 : (j + 1) * 128]
            f += 1
    for f in range(NF - 1, 4 * NY):
        wall[f] = jnp.zeros((2 * C, 128), BF16)
    pl.semaphore_wait(barrier, NZ - 1 + 2 * (NY - 1) + 1)

    sends = []

    def owe(ref, sem):
        sends.append(copy_to(ref, ref, sem, sem, **other).wait_send)

    def got(ref, sem):
        copy_to(ref, ref, sem, sem, **other).wait_recv()

    G = max(NZ // 8, 1)
    NG = NZ // G
    order = [0] + [(i + 1) // 2 if i % 2 else NG - i // 2 for i in range(1, NG)]

    def gather(slot, columns, sem, pair_sem):
        mine = slot(z, 1, y)

        def send(i, c):
            copy_to(mine, mine, sem.at[0], sem.at[1 + z // G], **at_z(zpeer(far_first(i)))).start()
            return c

        lax.fori_loop(0, NZ - 1, send, 0)
        owe(slot(0, NZ - 1, 0), sem.at[0])

        def finish():
            arrival = 2 + NG
            for i in range(NG):
                q = lax.rem(z // G + order[i], NG)
                n = G if i else G - 1
                if n:
                    got(slot(0, n, 0), sem.at[1 + q])
                group = slot(q * G, G, y)
                for j in (2, 1, 3):
                    copy_to(
                        group,
                        group,
                        sem.at[1 + NG],
                        sem.at[arrival + i],
                        **at_y(ypeer(j)),
                    ).start()
                copy_to(group, group, pair_sem.at[0], pair_sem.at[1], **other).start()
            for i in range(NG):
                q = lax.rem(z // G + order[i], NG)
                got(columns(0, G, NY - 1), sem.at[arrival + i])
                for j in (1, 3, 2):
                    group = slot(q * G, G, yfrom(j))
                    copy_to(group, group, pair_sem.at[0], pair_sem.at[1], **other).start()
            owe(columns(0, NZ, NY - 1), sem.at[1 + NG])
            everything = columns(0, NZ, NY)
            got(everything, pair_sem.at[1])
            owe(everything, pair_sem.at[0])

        return finish

    def gated(gate, up):
        return (gate * jax.nn.sigmoid(gate) * up).astype(BF16)

    def half(phase, hidden, wdt, meanwhile, residual):
        hx[phase, 0, 0:HID] = hidden
        hx[phase, 0, HID:] = jnp.zeros((128 - HID, R), BF16)
        hx[phase, 1, HID:] = jnp.zeros((128 - HID, R), BF16)
        units = pl.ds(0, HID)
        copy_to(
            hx.at[phase, 0, units],
            hx.at[phase, 1, units],
            hx_s.at[phase, 0],
            hx_s.at[phase, 1],
            **other,
        ).start()
        owe(hx.at[phase, 0, units], hx_s.at[phase, 0])
        far = [(i, pl.ds(lax.rem(z // G + o, NG) * G, G)) for i, o in enumerate(order[::-1])]
        got(wdx.at[phase], wd_s.at[phase, 1])
        got(hx.at[phase, 1, units], hx_s.at[phase, 1])
        pair_hidden = hx[phase].reshape(256, R)
        for slot, k in ((2, 2), (0, 1), (1, 3), (None, 4)):
            yy = lax.rem(y + k, NY)
            w = [wdt[t, yy].reshape(NZ * C, 128), wdx[phase, yy].reshape(NZ * C, 128)]
            both = dot(jnp.concatenate(w, axis=1), pair_hidden, 1, 0).reshape(NZ, C, R)
            if k == 4:
                break
            ysend[phase, slot] = both.astype(BF16)
            if k == 2:

                def direct(i, c):
                    kz = lax.rem(far_first(i), NZ)
                    zz = zpeer(kz)
                    copy_to(
                        ysend.at[phase, 2, zz],
                        zdirect.at[phase, kz],
                        rs_d.at[phase, 0],
                        rs_d.at[phase, 1],
                        kv=zz * NY + lax.rem(y + 2, NY),
                    ).start()
                    return c

                lax.fori_loop(0, NZ, direct, 0)
                continue
            for i, part in far:
                copy_to(
                    ysend.at[phase, slot, part],
                    yrecv.at[phase, slot, part],
                    rs_y.at[phase, 0],
                    rs_y.at[phase, 1 + i],
                    **at_y(yy),
                ).start()
        accf[phase] = both
        owe(ysend.at[phase, pl.ds(0, 2)], rs_y.at[phase, 0])
        owe(ysend.at[phase, 2], rs_d.at[phase, 0])
        for i, part in far:
            got(yrecv.at[phase, :, part], rs_y.at[phase, 1 + i])
            sums = accf[phase, part]
            for slot in range(2):
                sums = sums + yrecv[phase, slot, part].astype(F32)
            accf[phase, part] = sums
            zsend[phase, part] = sums.astype(BF16)
            for j in range(G):
                if i < NG - 1:
                    zz = part.start + j
                elif j:
                    zz = part.start + lax.rem(z + j, G)
                else:
                    continue
                copy_to(
                    zsend.at[phase, zz],
                    zrecv.at[phase, lax.rem(zz + NZ - z, NZ)],
                    rs_z.at[phase, 0],
                    rs_z.at[phase, 1],
                    **at_z(zz),
                ).start()
        landed = zrecv.at[phase, pl.ds(1, NZ - 1)]
        owe(landed, rs_z.at[phase, 0])
        meanwhile()
        total = accf[phase, z]
        got(landed, rs_z.at[phase, 1])
        got(zdirect.at[phase], rs_d.at[phase, 1])
        for k in range(NZ):
            total = total + zdirect[phase, k].astype(F32)
            if k:
                total = total + zrecv[phase, k].astype(F32)
        return (residual() + 0.5 * total).astype(BF16)

    def share_down(phase, wdt):
        copy_to(
            wdt.at[1 - t], wdx.at[phase], wd_s.at[phase, 0], wd_s.at[phase, 1], **other
        ).start()
        owe(wdx.at[phase], wd_s.at[phase, 0])

    gat1[z, y, t] = s0[...]
    finish = gather(
        lambda zz, n, yy: gat1.at[pl.ds(zz, n), yy, t],
        lambda zz, n, m: gat1.at[pl.ds(zz, n), pl.ds(0, m), t],
        ag.at[0],
        ag_t.at[0],
    )
    wsh[y] = wall[pl.ds(4 * y, 4)]
    share_down(0, wdt1)
    finish()
    all_rows = gat1[...].reshape(D, R)
    acc = dot(wgu1[...], all_rows, 1, 0)
    wide = all_rows.astype(F32)
    scale = lax.rsqrt(jnp.sum(wide * wide, axis=0, keepdims=True) / D + EPSILON)

    def share_weights():
        for k in range(1, NY):
            yy = ypeer(k)
            copy_to(wall.at[pl.ds(4 * yy, 4)], wsh.at[y], w_y.at[0], w_y.at[1], **at_y(yy)).start()
        load(14).wait()
        for k in range(1, NY):
            copy_to(wout, wog.at[y], wo_y.at[0], wo_y.at[1], **at_y(ypeer(k))).start()
        owe(wall.at[pl.ds(0, 4 * (NY - 1))], w_y.at[0])
        owe(wog.at[pl.ds(0, NY - 1)], wo_y.at[0])
        wog[y] = wout[...]

    hidden = gated(acc[:HID] * scale, acc[HID:] * scale)
    middle = half(0, hidden, wdt1, share_weights, lambda: s0[...].astype(F32))

    here = midg.at[2 * y + t]
    here[...] = middle
    for k in (2, 1, 3, 0):
        where = at_y(ypeer(k))
        copy_to(here, here, md.at[0], md.at[1], **where, **other).start()
        if k:
            copy_to(here, here, md.at[0], md.at[1], **where).start()
    most = midg.at[pl.ds(0, 2 * NY - 1)]
    owe(most, md.at[0])
    got(wsh.at[pl.ds(0, NY - 1)], w_y.at[1])
    got(most, md.at[1])

    turned = jnp.transpose(midg[...].astype(F32).reshape(NY * 2 * C, R))
    trn[...] = turned.reshape(2 * NY, NZ, 128)
    squares = jnp.sum(turned * turned, axis=1, keepdims=True)
    squares = squares * jnp.where(y == NY - 1, 1.0, 0.0)
    lhs = turned.astype(BF16)
    for c in range(4):
        part = dot(lhs, wsh[:, c].reshape(NY * 2 * C, 128), 1, 0)
        if c == 2:
            part = part + squares
        for yy in range(NY):
            for s in range(2):
                at = (yy * 2 + s) * NZ
                zs[pl.ds(yy * 8 + s * 4 + c, NZ, stride=32), :] = part[at : at + NZ]
    zsb[...] = zs[...].astype(BF16).reshape(NZ, NY, 8, 128)

    def send_sums(i, c):
        k = far_first(i)
        zz = zpeer(k)
        for j in (2, 1, 3, 0):
            yy = ypeer(j)
            there = {"kv": zz * NY + yy}
            copy_to(zsb.at[zz, yy], zrb.at[k * NY + y], pr_z.at[0], pr_z.at[1], **there).start()
        return c

    lax.fori_loop(0, NZ - 1, send_sums, 0)
    for j in (2, 1, 3):
        yy = ypeer(j)
        copy_to(zsb.at[z, yy], zrb.at[y], pr_z.at[0], pr_z.at[1], **at_y(yy)).start()
    zrb[y] = zsb[z, y]
    landed = zrb.at[pl.ds(0, NZ * NY - 1)]
    owe(landed, pr_z.at[0])
    for i in (1, 2, 13):
        load(i).wait()
    got(landed, pr_z.at[1])
    for yy in range(NY):
        total = zrb[yy].astype(F32)
        for k in range(1, NZ):
            total = total + zrb[k * NY + yy].astype(F32)
        ytot[yy] = total

    blocks = []
    columns = []
    for s in range(2):
        b = jnp.concatenate([ytot[yy, s * 4 : (s + 1) * 4] for yy in range(NY)], axis=0)
        b = b * lax.rsqrt(b[NF - 1 : NF] / D + EPSILON)
        blocks.append(b)
        logits = b[4:6]
        amounts = jnp.concatenate([dec[s : s + 1, 0:128], dec[s : s + 1, 128:256]], axis=0)
        sig = jnp.minimum(logits, 0.0) - jnp.log(1.0 + jnp.exp(-jnp.abs(logits)))
        decay = jnp.exp(sig / GATE_SOFTNESS - amounts)
        columns += [b[0:2] * 0.125, b[2:4], decay]
    columns.append(jnp.zeros((128 - 12, 128), F32))
    cols = jnp.transpose(jnp.concatenate(columns, axis=0))
    rows = []
    for s in range(2):
        for h in range(4):
            lo = (h % 2) * 64
            q, k_, a = (
                cols[lo : lo + 64, s * 6 + 2 * i + h // 2 : s * 6 + 2 * i + h // 2 + 1]
                for i in range(3)
            )
            b = blocks[s]
            state = a * old[s, h] + k_ * b[6 + h : 7 + h]
            newv[s, h] = state
            read = jnp.sum(q * state, axis=0, keepdims=True)
            normed = read * lax.rsqrt(jnp.mean(read * read, axis=1, keepdims=True) + EPSILON)
            o = b[10 + h : 11 + h]
            rows.append(normed * hg[h : h + 1] * (o * jax.nn.sigmoid(o)))
    mg[z] = jnp.concatenate(rows, axis=0).astype(BF16)

    def send_heads(i, c):
        zz = zpeer(far_first(i))
        copy_to(mg.at[z], mg.at[z], mh.at[0], mh.at[1], **at_z(zz)).start()
        return c

    lax.fori_loop(0, NZ - 1, send_heads, 0)
    owe(mg.at[pl.ds(0, NZ - 1)], mh.at[0])
    out_copy = pltpu.make_async_copy(newv, new, ld.at[0])
    out_copy.start()
    sends.append(out_copy.wait)
    for i in (15, 16, 17, 18):
        load(i).wait()
    turn(wdt2, wd2)
    fold(wgu2, wg2, wu2, g2)
    share_down(1, wdt2)
    got(wog.at[pl.ds(0, NY - 1)], wo_y.at[1])
    got(mg.at[pl.ds(0, NZ - 1)], mh.at[1])
    mgf[...] = mg[...].astype(F32).reshape(NZ * 8, 128)
    heads = []
    for h in range(4):
        pieces = [mgf[pl.ds(s * 4 + h, NZ, stride=8), :] for s in range(2)]
        heads.append(jnp.concatenate(pieces, axis=0))
    mixed = jnp.concatenate(heads, axis=1).astype(BF16)
    product = dot(mixed, wog[...].reshape(NY * 2 * C, 512), 1, 1).astype(BF16)
    pj[...] = product.reshape(2, NZ, NY * 2 * C)
    copy_to(pj.at[1 - t], pjr, fin_s.at[0], fin_s.at[1], **other).start()
    owe(pjr, fin_s.at[0])
    got(pjr, fin_s.at[1])
    attention = pj[t].astype(F32) + pjr[...].astype(F32)

    gat2[z, y, t] = (trn[2 * y + t] + attention).astype(BF16)
    gather(
        lambda zz, n, yy: gat2.at[pl.ds(zz, n), yy, t],
        lambda zz, n, m: gat2.at[pl.ds(zz, n), pl.ds(0, m), t],
        ag.at[1],
        ag_t.at[1],
    )()
    all_rows = jnp.concatenate([gat2[i].reshape(R, NY * 2 * C) for i in range(NZ)], axis=1)
    acc = dot(all_rows, wgu2[...], 1, 1)
    wide = all_rows.astype(F32)
    scale = lax.rsqrt(jnp.sum(wide * wide, axis=1, keepdims=True) / D + EPSILON)
    acc = jnp.transpose(acc * scale)

    def own_columns():
        block = gat2[z].astype(F32).reshape(R, NY * 2 * C)
        aft[...] = jnp.transpose(block).reshape(2 * NY, C, R)

    hidden = gated(acc[:HID], acc[HID : 2 * HID])
    result = half(1, hidden, wdt2, own_columns, lambda: aft[2 * y + t])
    outT[...] = dot(result, perm, 1, 1).astype(BF16)
    for wait in sends:
        wait()


def write_out(outT, new, outT_ref, new_ref, o_v, n_v, sem):
    parts = new.shape[0]
    moves = [(outT, o_v, outT_ref)] + [(new.at[i], n_v.at[i], new_ref.at[i]) for i in range(parts)]
    ins = [pltpu.make_async_copy(a, v, sem.at[0, i]) for i, (a, v, _) in enumerate(moves)]
    outs = [pltpu.make_async_copy(v, b, sem.at[1, i]) for i, (_, v, b) in enumerate(moves)]
    for c in ins:
        c.start()
    for a, b in zip(ins, outs):
        a.wait()
        b.start()
    for c in outs:
        c.wait()


def body(
    stream,
    old_state,
    decay_amounts,
    first_gain,
    first_gate,
    first_up,
    first_down,
    mixer_gain,
    query_weight,
    key_weight,
    decay_weight,
    value_weight,
    output_gate_weight,
    head_gain,
    output_weight,
    second_gain,
    second_gate,
    second_up,
    second_down,
):
    NZ = lax.axis_size("kv") // NY
    R = 2 * NY * NZ
    D = NY * NZ * 2 * C
    NG = NZ // max(NZ // 8, 1)
    V = pltpu.VMEM
    S = pltpu.SemaphoreType.DMA
    arrays = (
        stream.T,
        old_state,
        decay_amounts,
        first_gain.reshape(1, D),
        first_gate.T,
        first_up.T,
        first_down,
        mixer_gain.reshape(1, 2 * C),
        query_weight,
        key_weight,
        decay_weight,
        value_weight,
        output_gate_weight,
        head_gain.reshape(4, 128),
        output_weight.T,
        second_gain.reshape(1, D),
        second_gate.T,
        second_up.T,
        second_down,
    )
    outT, new = pl.pallas_call(
        functools.partial(kernel, NZ, first_gate.shape[1]),
        out_shape=(
            jax.ShapeDtypeStruct((C, R), BF16),
            jax.ShapeDtypeStruct(old_state.shape, F32),
        ),
        in_specs=[pl.BlockSpec(memory_space=pl.ANY)] * 19,
        out_specs=[pl.BlockSpec(memory_space=pltpu.VMEM), pl.BlockSpec(memory_space=pl.ANY)],
        scratch_shapes=[V(a.shape, a.dtype) for a in arrays]
        + [
            V(old_state.shape, F32),
            V((NZ, NY, 2, C, R), BF16),
            V((NZ, NY, 2, NZ, NY * 2 * C), BF16),
            V((2 * HID, D), BF16),
            V((128, D), BF16),
            V((2, NY, NZ, C, 128), BF16),
            V((2, NY, NZ, C, 128), BF16),
            V((C, R), BF16),
            V((2, 2, 128, R), BF16),
            V((2, NY, NZ, C, 128), BF16),
            V((2, 3, NZ, C, R), BF16),
            V((2, 2, NZ, C, R), BF16),
            V((2, NZ, C, R), BF16),
            V((2, NZ, C, R), F32),
            V((2, NZ, C, R), BF16),
            V((2, NZ, C, R), BF16),
            V((2 * NY, C, R), BF16),
            V((4 * NY, 2 * C, 128), BF16),
            V((NY, 4, 2 * C, 128), BF16),
            V((NY, 2 * C, 512), BF16),
            V((2 * NY, NZ, 128), F32),
            V((NZ * 32, 128), F32),
            V((NZ, NY, 8, 128), BF16),
            V((NZ * NY, 8, 128), BF16),
            V((NY, 8, 128), F32),
            V((NZ, 8, 128), BF16),
            V((NZ * 8, 128), F32),
            V((2, NZ, NY * 2 * C), BF16),
            V((NZ, NY * 2 * C), BF16),
            V((2 * NY, C, R), F32),
            S((19,)),
            S((2, 2 + 2 * NG)),
            S((2, 2)),
            S((2, 2)),
            S((2, 2)),
            S((2, 1 + NG)),
            S((2, 2)),
            S((2, 2)),
            S((2,)),
            S((2,)),
            S((2,)),
            S((2,)),
            S((2,)),
            S((2,)),
        ],
        compiler_params=pltpu.CompilerParams(collective_id=0, has_side_effects=True),
        name="layer",
    )(*arrays)
    outT, new = pl.pallas_call(
        write_out,
        out_shape=(
            jax.ShapeDtypeStruct(outT.shape, BF16),
            jax.ShapeDtypeStruct(new.shape, F32),
        ),
        in_specs=[pl.BlockSpec(memory_space=pl.ANY)] * 2,
        out_specs=[pl.BlockSpec(memory_space=pl.ANY)] * 2,
        scratch_shapes=[V(outT.shape, BF16), V(new.shape, F32), S((2, 1 + new.shape[0]))],
        name="write_out",
    )(outT, new)
    return outT.T, new


def solution(mesh):
    in_specs = (
        P("dp", ("kv", "tp")),
        P(("dp", "kv"), "tp", None, None),
        P(("dp", "kv"), "tp"),
        P(),
        P(None, ("kv", "tp")),
        P(None, ("kv", "tp")),
        P(("kv", "tp"), None),
        P("kv"),
        P("kv", "tp"),
        P("kv", "tp"),
        P("kv", "tp"),
        P("kv", "tp"),
        P("kv", "tp"),
        P("tp"),
        P("tp", "kv"),
        P(),
        P(None, ("kv", "tp")),
        P(None, ("kv", "tp")),
        P(("kv", "tp"), None),
    )
    out_specs = (P("dp", ("kv", "tp")), P(("dp", "kv"), "tp", None, None))
    return jax.shard_map(body, mesh=mesh, in_specs=in_specs, out_specs=out_specs, check_vma=False)
```

```python
import functools

import jax
import jax.numpy as jnp
from jax import lax
from jax.experimental import pallas as pl
from jax.experimental.pallas import tpu as pltpu
from jax.sharding import PartitionSpec as P

EPSILON = 1e-06
GATE_SOFTNESS = 16.0
NY = 4
C = 16
HID = 48
NF = 15
F32 = jnp.float32
BF16 = jnp.bfloat16


def copy_to(src, dst, send, recv, **where):
    return pltpu.make_async_remote_copy(
        src_ref=src,
        dst_ref=dst,
        send_sem=send,
        recv_sem=recv,
        device_id=where,
        device_id_type=pl.DeviceIdType.MESH,
    )


def dot(a, b, ca, cb):
    return lax.dot_general(a, b, (((ca,), (cb,)), ((), ())), preferred_element_type=F32)


def kernel(NZ, FFL, *refs):
    hbm = refs[:19]
    outT, new = refs[19:21]
    local = refs[21:40]
    (
        newv,
        gat1,
        gat2,
        wgu1,
        wgu2,
        wdt1,
        wdt2,
        s0,
        hx,
        wdx,
        ysend,
        yrecv,
        zdirect,
        accf,
        zsend,
        zrecv,
        midg,
        wall,
        wsh,
        wog,
        trn,
        zs,
        zsb,
        zrb,
        ytot,
        mg,
        mgf,
        pj,
        pjr,
        aft,
        ld,
        ag,
        ag_t,
        hx_s,
        wd_s,
        rs_y,
        rs_d,
        rs_z,
        md,
        w_y,
        wo_y,
        pr_z,
        mh,
        fin_s,
    ) = refs[40:]
    (
        sT,
        old,
        dec,
        g1,
        wg1,
        wu1,
        wd1,
        gm,
        wq,
        wk,
        wz,
        wv,
        wo,
        hg,
        wout,
        g2,
        wg2,
        wu2,
        wd2,
    ) = local
    kv = lax.axis_index("kv")
    t = lax.axis_index("tp")
    z = kv // NY
    y = kv % NY
    R = 2 * NY * NZ
    D = NZ * NY * 2 * C

    def zpeer(k):
        return lax.rem(z + k, NZ)

    def ypeer(k):
        return lax.rem(y + k, NY)

    def yfrom(k):
        return lax.rem(y + NY - k, NY)

    def at_z(zz):
        return {"kv": zz * NY + y}

    def at_y(yy):
        return {"kv": z * NY + yy}

    other = {"tp": 1 - t}

    def far_first(i):
        return NZ // 2 + (1 - 2 * lax.rem(i, 2)) * ((i + 1) // 2)

    barrier = pltpu.get_barrier_semaphore()

    def greet(**where):
        pl.semaphore_signal(
            barrier, inc=1, device_id=where, device_id_type=pl.DeviceIdType.MESH
        )

    def greet_z(i, c):
        greet(**at_z(zpeer(far_first(i))))
        return c

    lax.fori_loop(0, NZ - 1, greet_z, 0)
    for k in range(1, NY):
        greet(**at_y(ypeer(k)))
        greet(**at_y(ypeer(k)), **other)
    greet(**other)

    def load(i):
        return pltpu.make_async_copy(hbm[i], local[i], ld.at[i])

    for i in (0, 3, 4, 5, 6, 7, 8, 9, 10, 11, 12, 15, 16, 17, 18, 1, 2, 13, 14):
        load(i).start()

    seq = lax.broadcasted_iota(jnp.int32, (R, R), 0)
    lane = lax.broadcasted_iota(jnp.int32, (R, R), 1)
    home = (lane % NZ) * (2 * NY) + (lane // (2 * NZ)) * 2 + (lane // NZ) % 2
    perm = jnp.where(seq == home, 1.0, 0.0).astype(BF16)
    load(0).wait()
    s0[...] = dot(sT[...], perm, 1, 0).astype(BF16)

    def fold(wgu, wg, wu, gain):
        row = gain[...]
        pad = jnp.zeros((HID - FFL, D), F32)
        for part, w in enumerate((wg, wu)):
            scaled = jnp.concatenate([w[...].astype(F32) * row, pad], axis=0)
            wgu[part * HID : (part + 1) * HID, :] = scaled.astype(BF16)
        if wgu.shape[0] > 2 * HID:
            wgu[2 * HID :, :] = jnp.zeros((wgu.shape[0] - 2 * HID, D), BF16)

    def turn(wdt, wd):
        width = NY * 2 * C
        for b in range(NZ):
            block = wd[:, b * width : (b + 1) * width].astype(F32)
            block = jnp.concatenate([block, jnp.zeros((128 - FFL, width), F32)], axis=0)
            turned = jnp.transpose(block).astype(BF16).reshape(NY, 2, C, 128)
            for p in range(2):
                for yy in range(NY):
                    wdt[p, yy, b] = turned[yy, p]

    for i in (3, 4, 5):
        load(i).wait()
    fold(wgu1, wg1, wu1, g1)
    load(6).wait()
    turn(wdt1, wd1)
    for i in range(7, 13):
        load(i).wait()
    eye = lax.broadcasted_iota(jnp.int32, (2 * C, 2 * C), 0) == lax.broadcasted_iota(
        jnp.int32, (2 * C, 2 * C), 1
    )
    gain_col = jnp.sum(
        jnp.where(eye, jnp.broadcast_to(gm[...], (2 * C, 2 * C)), 0.0), axis=1, keepdims=True
    )
    f = 0
    for w in (wq, wk, wz, wv, wo):
        scaled = (w[...].astype(F32) * gain_col).astype(BF16)
        for j in range(w.shape[1] // 128):
            wall[f] = scaled[:, j * 128 : (j + 1) * 128]
            f += 1
    for f in range(NF - 1, 4 * NY):
        wall[f] = jnp.zeros((2 * C, 128), BF16)
    pl.semaphore_wait(barrier, NZ - 1 + 2 * (NY - 1) + 1)

    sends = []

    def owe(ref, sem):
        sends.append(copy_to(ref, ref, sem, sem, **other).wait_send)

    def got(ref, sem):
        copy_to(ref, ref, sem, sem, **other).wait_recv()

    G = max(NZ // 8, 1)
    NG = NZ // G
    order = [0] + [(i + 1) // 2 if i % 2 else NG - i // 2 for i in range(1, NG)]

    def gather(slot, columns, sem, pair_sem):
        mine = slot(z, 1, y)

        def send(i, c):
            copy_to(mine, mine, sem.at[0], sem.at[1 + z // G], **at_z(zpeer(far_first(i)))).start()
            return c

        lax.fori_loop(0, NZ - 1, send, 0)
        owe(slot(0, NZ - 1, 0), sem.at[0])

        def finish():
            arrival = 2 + NG
            for i in range(NG):
                q = lax.rem(z // G + order[i], NG)
                n = G if i else G - 1
                if n:
                    got(slot(0, n, 0), sem.at[1 + q])
                group = slot(q * G, G, y)
                for j in (2, 1, 3):
                    copy_to(
                        group,
                        group,
                        sem.at[1 + NG],
                        sem.at[arrival + i],
                        **at_y(ypeer(j)),
                    ).start()
                copy_to(group, group, pair_sem.at[0], pair_sem.at[1], **other).start()
            for i in range(NG):
                q = lax.rem(z // G + order[i], NG)
                got(columns(0, G, NY - 1), sem.at[arrival + i])
                for j in (1, 3, 2):
                    group = slot(q * G, G, yfrom(j))
                    copy_to(group, group, pair_sem.at[0], pair_sem.at[1], **other).start()
            owe(columns(0, NZ, NY - 1), sem.at[1 + NG])
            everything = columns(0, NZ, NY)
            got(everything, pair_sem.at[1])
            owe(everything, pair_sem.at[0])

        return finish

    def gated(gate, up):
        return (gate * jax.nn.sigmoid(gate) * up).astype(BF16)

    def half(phase, hidden, wdt, meanwhile, residual):
        hx[phase, 0, 0:HID] = hidden
        hx[phase, 0, HID:] = jnp.zeros((128 - HID, R), BF16)
        hx[phase, 1, HID:] = jnp.zeros((128 - HID, R), BF16)
        units = pl.ds(0, HID)
        copy_to(
            hx.at[phase, 0, units],
            hx.at[phase, 1, units],
            hx_s.at[phase, 0],
            hx_s.at[phase, 1],
            **other,
        ).start()
        owe(hx.at[phase, 0, units], hx_s.at[phase, 0])
        far = [(i, pl.ds(lax.rem(z // G + o, NG) * G, G)) for i, o in enumerate(order[::-1])]
        got(wdx.at[phase], wd_s.at[phase, 1])
        got(hx.at[phase, 1, units], hx_s.at[phase, 1])
        pair_hidden = hx[phase].reshape(256, R)
        for slot, k in ((2, 2), (0, 1), (1, 3), (None, 4)):
            yy = lax.rem(y + k, NY)
            w = [wdt[t, yy].reshape(NZ * C, 128), wdx[phase, yy].reshape(NZ * C, 128)]
            both = dot(jnp.concatenate(w, axis=1), pair_hidden, 1, 0).reshape(NZ, C, R)
            if k == 4:
                break
            ysend[phase, slot] = both.astype(BF16)
            if k == 2:

                def direct(i, c):
                    kz = lax.rem(far_first(i), NZ)
                    zz = zpeer(kz)
                    copy_to(
                        ysend.at[phase, 2, zz],
                        zdirect.at[phase, kz],
                        rs_d.at[phase, 0],
                        rs_d.at[phase, 1],
                        kv=zz * NY + lax.rem(y + 2, NY),
                    ).start()
                    return c

                lax.fori_loop(0, NZ, direct, 0)
                continue
            for i, part in far:
                copy_to(
                    ysend.at[phase, slot, part],
                    yrecv.at[phase, slot, part],
                    rs_y.at[phase, 0],
                    rs_y.at[phase, 1 + i],
                    **at_y(yy),
                ).start()
        accf[phase] = both
        owe(ysend.at[phase, pl.ds(0, 2)], rs_y.at[phase, 0])
        owe(ysend.at[phase, 2], rs_d.at[phase, 0])
        for i, part in far:
            got(yrecv.at[phase, :, part], rs_y.at[phase, 1 + i])
            sums = accf[phase, part]
            for slot in range(2):
                sums = sums + yrecv[phase, slot, part].astype(F32)
            accf[phase, part] = sums
            zsend[phase, part] = sums.astype(BF16)
            for j in range(G):
                if i < NG - 1:
                    zz = part.start + j
                elif j:
                    zz = part.start + lax.rem(z + j, G)
                else:
                    continue
                copy_to(
                    zsend.at[phase, zz],
                    zrecv.at[phase, lax.rem(zz + NZ - z, NZ)],
                    rs_z.at[phase, 0],
                    rs_z.at[phase, 1],
                    **at_z(zz),
                ).start()
        landed = zrecv.at[phase, pl.ds(1, NZ - 1)]
        owe(landed, rs_z.at[phase, 0])
        meanwhile()
        total = accf[phase, z]
        got(landed, rs_z.at[phase, 1])
        got(zdirect.at[phase], rs_d.at[phase, 1])
        for k in range(NZ):
            total = total + zdirect[phase, k].astype(F32)
            if k:
                total = total + zrecv[phase, k].astype(F32)
        return (residual() + 0.5 * total).astype(BF16)

    def share_down(phase, wdt):
        copy_to(
            wdt.at[1 - t], wdx.at[phase], wd_s.at[phase, 0], wd_s.at[phase, 1], **other
        ).start()
        owe(wdx.at[phase], wd_s.at[phase, 0])

    gat1[z, y, t] = s0[...]
    finish = gather(
        lambda zz, n, yy: gat1.at[pl.ds(zz, n), yy, t],
        lambda zz, n, m: gat1.at[pl.ds(zz, n), pl.ds(0, m), t],
        ag.at[0],
        ag_t.at[0],
    )
    wsh[y] = wall[pl.ds(4 * y, 4)]
    share_down(0, wdt1)
    finish()
    all_rows = gat1[...].reshape(D, R)
    acc = dot(wgu1[...], all_rows, 1, 0)
    wide = all_rows.astype(F32)
    scale = lax.rsqrt(jnp.sum(wide * wide, axis=0, keepdims=True) / D + EPSILON)

    def share_weights():
        for k in range(1, NY):
            yy = ypeer(k)
            copy_to(wall.at[pl.ds(4 * yy, 4)], wsh.at[y], w_y.at[0], w_y.at[1], **at_y(yy)).start()
        load(14).wait()
        for k in range(1, NY):
            copy_to(wout, wog.at[y], wo_y.at[0], wo_y.at[1], **at_y(ypeer(k))).start()
        owe(wall.at[pl.ds(0, 4 * (NY - 1))], w_y.at[0])
        owe(wog.at[pl.ds(0, NY - 1)], wo_y.at[0])
        wog[y] = wout[...]

    hidden = gated(acc[:HID] * scale, acc[HID:] * scale)
    middle = half(0, hidden, wdt1, share_weights, lambda: s0[...].astype(F32))

    here = midg.at[2 * y + t]
    here[...] = middle
    for k in range(NY):
        where = at_y(ypeer(k))
        copy_to(here, here, md.at[0], md.at[1], **where, **other).start()
        if k:
            copy_to(here, here, md.at[0], md.at[1], **where).start()
    most = midg.at[pl.ds(0, 2 * NY - 1)]
    owe(most, md.at[0])
    got(wsh.at[pl.ds(0, NY - 1)], w_y.at[1])
    got(most, md.at[1])

    turned = jnp.transpose(midg[...].astype(F32).reshape(NY * 2 * C, R))
    trn[...] = turned.reshape(2 * NY, NZ, 128)
    squares = jnp.sum(turned * turned, axis=1, keepdims=True)
    squares = squares * jnp.where(y == NY - 1, 1.0, 0.0)
    lhs = turned.astype(BF16)
    for c in range(4):
        part = dot(lhs, wsh[:, c].reshape(NY * 2 * C, 128), 1, 0)
        if c == 2:
            part = part + squares
        for yy in range(NY):
            for s in range(2):
                at = (yy * 2 + s) * NZ
                zs[pl.ds(yy * 8 + s * 4 + c, NZ, stride=32), :] = part[at : at + NZ]
    zsb[...] = zs[...].astype(BF16).reshape(NZ, NY, 8, 128)

    def send_sums(i, c):
        k = far_first(i)
        zz = zpeer(k)
        for j in (2, 1, 3, 0):
            yy = ypeer(j)
            there = {"kv": zz * NY + yy}
            copy_to(zsb.at[zz, yy], zrb.at[k * NY + y], pr_z.at[0], pr_z.at[1], **there).start()
        return c

    lax.fori_loop(0, NZ - 1, send_sums, 0)
    for j in (2, 1, 3):
        yy = ypeer(j)
        copy_to(zsb.at[z, yy], zrb.at[y], pr_z.at[0], pr_z.at[1], **at_y(yy)).start()
    zrb[y] = zsb[z, y]
    landed = zrb.at[pl.ds(0, NZ * NY - 1)]
    owe(landed, pr_z.at[0])
    for i in (1, 2, 13):
        load(i).wait()
    got(landed, pr_z.at[1])
    for yy in range(NY):
        total = zrb[yy].astype(F32)
        for k in range(1, NZ):
            total = total + zrb[k * NY + yy].astype(F32)
        ytot[yy] = total

    blocks = []
    columns = []
    for s in range(2):
        b = jnp.concatenate([ytot[yy, s * 4 : (s + 1) * 4] for yy in range(NY)], axis=0)
        b = b * lax.rsqrt(b[NF - 1 : NF] / D + EPSILON)
        blocks.append(b)
        logits = b[4:6]
        amounts = jnp.concatenate([dec[s : s + 1, 0:128], dec[s : s + 1, 128:256]], axis=0)
        sig = jnp.minimum(logits, 0.0) - jnp.log(1.0 + jnp.exp(-jnp.abs(logits)))
        decay = jnp.exp(sig / GATE_SOFTNESS - amounts)
        columns += [b[0:2] * 0.125, b[2:4], decay]
    columns.append(jnp.zeros((128 - 12, 128), F32))
    cols = jnp.transpose(jnp.concatenate(columns, axis=0))
    rows = []
    for s in range(2):
        for h in range(4):
            lo = (h % 2) * 64
            q, k_, a = (
                cols[lo : lo + 64, s * 6 + 2 * i + h // 2 : s * 6 + 2 * i + h // 2 + 1]
                for i in range(3)
            )
            b = blocks[s]
            state = a * old[s, h] + k_ * b[6 + h : 7 + h]
            newv[s, h] = state
            read = jnp.sum(q * state, axis=0, keepdims=True)
            normed = read * lax.rsqrt(jnp.mean(read * read, axis=1, keepdims=True) + EPSILON)
            o = b[10 + h : 11 + h]
            rows.append(normed * hg[h : h + 1] * (o * jax.nn.sigmoid(o)))
    mg[z] = jnp.concatenate(rows, axis=0).astype(BF16)

    def send_heads(i, c):
        zz = zpeer(far_first(i))
        copy_to(mg.at[z], mg.at[z], mh.at[0], mh.at[1], **at_z(zz)).start()
        return c

    lax.fori_loop(0, NZ - 1, send_heads, 0)
    owe(mg.at[pl.ds(0, NZ - 1)], mh.at[0])
    out_copy = pltpu.make_async_copy(newv, new, ld.at[0])
    out_copy.start()
    sends.append(out_copy.wait)
    for i in (15, 16, 17, 18):
        load(i).wait()
    fold(wgu2, wg2, wu2, g2)
    turn(wdt2, wd2)
    got(wog.at[pl.ds(0, NY - 1)], wo_y.at[1])
    got(mg.at[pl.ds(0, NZ - 1)], mh.at[1])
    share_down(1, wdt2)
    mgf[...] = mg[...].astype(F32).reshape(NZ * 8, 128)
    heads = []
    for h in range(4):
        pieces = [mgf[pl.ds(s * 4 + h, NZ, stride=8), :] for s in range(2)]
        heads.append(jnp.concatenate(pieces, axis=0))
    mixed = jnp.concatenate(heads, axis=1).astype(BF16)
    product = dot(mixed, wog[...].reshape(NY * 2 * C, 512), 1, 1).astype(BF16)
    pj[...] = product.reshape(2, NZ, NY * 2 * C)
    copy_to(pj.at[1 - t], pjr, fin_s.at[0], fin_s.at[1], **other).start()
    owe(pjr, fin_s.at[0])
    got(pjr, fin_s.at[1])
    attention = pj[t].astype(F32) + pjr[...].astype(F32)

    gat2[z, y, t] = (trn[2 * y + t] + attention).astype(BF16)
    gather(
        lambda zz, n, yy: gat2.at[pl.ds(zz, n), yy, t],
        lambda zz, n, m: gat2.at[pl.ds(zz, n), pl.ds(0, m), t],
        ag.at[1],
        ag_t.at[1],
    )()
    all_rows = jnp.concatenate([gat2[i].reshape(R, NY * 2 * C) for i in range(NZ)], axis=1)
    acc = dot(all_rows, wgu2[...], 1, 1)
    wide = all_rows.astype(F32)
    scale = lax.rsqrt(jnp.sum(wide * wide, axis=1, keepdims=True) / D + EPSILON)
    acc = jnp.transpose(acc * scale)

    def own_columns():
        block = gat2[z].astype(F32).reshape(R, NY * 2 * C)
        aft[...] = jnp.transpose(block).reshape(2 * NY, C, R)

    hidden = gated(acc[:HID], acc[HID : 2 * HID])
    result = half(1, hidden, wdt2, own_columns, lambda: aft[2 * y + t])
    outT[...] = dot(result, perm, 1, 1).astype(BF16)
    for wait in sends:
        wait()


def write_out(outT, new, outT_ref, new_ref, o_v, n_v, sem):
    moves = [(outT, o_v, outT_ref)]
    for i in range(new.shape[0]):
        for h in range(new.shape[1]):
            moves.append((new.at[i, h], n_v.at[i, h], new_ref.at[i, h]))
    ins = [pltpu.make_async_copy(a, v, sem.at[0, i]) for i, (a, v, _) in enumerate(moves)]
    outs = [pltpu.make_async_copy(v, b, sem.at[1, i]) for i, (_, v, b) in enumerate(moves)]
    for c in ins:
        c.start()
    for a, b in zip(ins, outs):
        a.wait()
        b.start()
    for c in outs:
        c.wait()


def body(
    stream,
    old_state,
    decay_amounts,
    first_gain,
    first_gate,
    first_up,
    first_down,
    mixer_gain,
    query_weight,
    key_weight,
    decay_weight,
    value_weight,
    output_gate_weight,
    head_gain,
    output_weight,
    second_gain,
    second_gate,
    second_up,
    second_down,
):
    NZ = lax.axis_size("kv") // NY
    R = 2 * NY * NZ
    D = NY * NZ * 2 * C
    NG = NZ // max(NZ // 8, 1)
    V = pltpu.VMEM
    S = pltpu.SemaphoreType.DMA
    arrays = (
        stream.T,
        old_state,
        decay_amounts,
        first_gain.reshape(1, D),
        first_gate.T,
        first_up.T,
        first_down,
        mixer_gain.reshape(1, 2 * C),
        query_weight,
        key_weight,
        decay_weight,
        value_weight,
        output_gate_weight,
        head_gain.reshape(4, 128),
        output_weight.T,
        second_gain.reshape(1, D),
        second_gate.T,
        second_up.T,
        second_down,
    )
    outT, new = pl.pallas_call(
        functools.partial(kernel, NZ, first_gate.shape[1]),
        out_shape=(
            jax.ShapeDtypeStruct((C, R), BF16),
            jax.ShapeDtypeStruct(old_state.shape, F32),
        ),
        in_specs=[pl.BlockSpec(memory_space=pl.ANY)] * 19,
        out_specs=[pl.BlockSpec(memory_space=pltpu.VMEM), pl.BlockSpec(memory_space=pl.ANY)],
        scratch_shapes=[V(a.shape, a.dtype) for a in arrays]
        + [
            V(old_state.shape, F32),
            V((NZ, NY, 2, C, R), BF16),
            V((NZ, NY, 2, NZ, NY * 2 * C), BF16),
            V((2 * HID, D), BF16),
            V((128, D), BF16),
            V((2, NY, NZ, C, 128), BF16),
            V((2, NY, NZ, C, 128), BF16),
            V((C, R), BF16),
            V((2, 2, 128, R), BF16),
            V((2, NY, NZ, C, 128), BF16),
            V((2, 3, NZ, C, R), BF16),
            V((2, 2, NZ, C, R), BF16),
            V((2, NZ, C, R), BF16),
            V((2, NZ, C, R), F32),
            V((2, NZ, C, R), BF16),
            V((2, NZ, C, R), BF16),
            V((2 * NY, C, R), BF16),
            V((4 * NY, 2 * C, 128), BF16),
            V((NY, 4, 2 * C, 128), BF16),
            V((NY, 2 * C, 512), BF16),
            V((2 * NY, NZ, 128), F32),
            V((NZ * 32, 128), F32),
            V((NZ, NY, 8, 128), BF16),
            V((NZ * NY, 8, 128), BF16),
            V((NY, 8, 128), F32),
            V((NZ, 8, 128), BF16),
            V((NZ * 8, 128), F32),
            V((2, NZ, NY * 2 * C), BF16),
            V((NZ, NY * 2 * C), BF16),
            V((2 * NY, C, R), F32),
            S((19,)),
            S((2, 2 + 2 * NG)),
            S((2, 2)),
            S((2, 2)),
            S((2, 2)),
            S((2, 1 + NG)),
            S((2, 2)),
            S((2, 2)),
            S((2,)),
            S((2,)),
            S((2,)),
            S((2,)),
            S((2,)),
            S((2,)),
        ],
        compiler_params=pltpu.CompilerParams(collective_id=0, has_side_effects=True),
        name="layer",
    )(*arrays)
    outT, new = pl.pallas_call(
        write_out,
        out_shape=(
            jax.ShapeDtypeStruct(outT.shape, BF16),
            jax.ShapeDtypeStruct(new.shape, F32),
        ),
        in_specs=[pl.BlockSpec(memory_space=pl.ANY)] * 2,
        out_specs=[pl.BlockSpec(memory_space=pl.ANY)] * 2,
        scratch_shapes=[V(outT.shape, BF16), V(new.shape, F32), S((2, 1 + new.shape[0] * new.shape[1]))],
        name="write_out",
    )(outT, new)
    return outT.T, new


def solution(mesh):
    in_specs = (
        P("dp", ("kv", "tp")),
        P(("dp", "kv"), "tp", None, None),
        P(("dp", "kv"), "tp"),
        P(),
        P(None, ("kv", "tp")),
        P(None, ("kv", "tp")),
        P(("kv", "tp"), None),
        P("kv"),
        P("kv", "tp"),
        P("kv", "tp"),
        P("kv", "tp"),
        P("kv", "tp"),
        P("kv", "tp"),
        P("tp"),
        P("tp", "kv"),
        P(),
        P(None, ("kv", "tp")),
        P(None, ("kv", "tp")),
        P(("kv", "tp"), None),
    )
    out_specs = (P("dp", ("kv", "tp")), P(("dp", "kv"), "tp", None, None))
    return jax.shard_map(body, mesh=mesh, in_specs=in_specs, out_specs=out_specs, check_vma=False)
```
